256 devices in a mesh: sp: 16 (over y, x), tp: 16 (over z, core).
Axes of the slice: x: 4, y: 4, z: 8, core: 2. Of those that a mesh axis runs over, the one named last changes fastest.
Arguments:
- queries: bfloat16 [32768, 2048], P('sp', 'tp'), may hold values from -160 to 160
- key_heads: bfloat16 [32768, 512], P('sp'), may hold values from -8 to 8
- value_heads: bfloat16 [32768, 512], P('sp'), may hold values from -4 to 4
- sink_logit: float32 [16], P('tp'), may hold values from -2 to 7
- out_weight: bfloat16 [2048, 2048], P('tp'), may hold values from -0.125 to 0.125
- residual: bfloat16 [32768, 2048], P(('sp', 'tp')), may hold values from -6 to 6
- mixer_gain: float32 [2048], replicated, may hold values from 0.1 to 1.9
- expert_gain: float32 [2048], replicated, may hold values from 0.1 to 1.9
- route_group: int32 [32768], P(('sp', 'tp')), may hold values from 0 to 15, as said below
- route_member: int32 [32768, 2], P(('sp', 'tp')), may hold values from 0 to 2, as said below
- route_weight: bfloat16 [32768, 2], P(('sp', 'tp')), may hold values from 0.19921875 to 1
- gate_weight: bfloat16 [48, 2048, 2048], P('sp', None, 'tp'), may hold values from -0.125 to 0.125
- up_weight: bfloat16 [48, 2048, 2048], P('sp', None, 'tp'), may hold values from -0.125 to 0.125
- down_weight: bfloat16 [48, 2048, 2048], P('sp', 'tp'), may hold values from -0.125 to 0.125
Outputs:
- output: bfloat16 [32768, 2048], P(('sp', 'tp'))
The draws below stay inside these ranges and needn't reach their ends.
Inputs may be any that keep to these rules, and one draw needn't show every extreme that they name: `route_group`: among the tokens of one device, at most 10 name one group; in every draw one group is named by exactly 10 tokens of every device. `route_member`: the two entries of a token are different members of its group.
All inputs are finite; a program needn't handle non-finite values.
Results may differ from the reference program's by a relative error of at most 0.018.
Values may be sent and summed in bfloat16 or wider, within the bound.
A program may use at most 128 MiB of HBM per device.

```python
import jax
import jax.numpy as jnp
from jax import lax

D = 2048
HEADS = 16
KV_HEADS = 4
HEAD_DIM = 128
WINDOW = 128
BLOCK = 128
EXP_HID = 2048
GROUP_EXPERTS = 3
TOP = 2
TOK_DEV = 128
TOKENS = 32768
GROUPS = 16
EXPERTS = 48
GROUP_CAP = 10
N_TP = 16


def draw_key_heads(key, part):
    return jnp.clip(jax.random.normal(jax.random.fold_in(key, 37), (TOKENS, KV_HEADS * HEAD_DIM), jnp.float32), -4.0, 4.0).astype(jnp.bfloat16)


def draw_queries(key, part):
    drawn_rows = jnp.clip(jax.random.normal(jax.random.fold_in(key, 41), (TOKENS, HEADS * HEAD_DIM), jnp.float32), -4.0, 4.0)
    return drawn_rows.astype(jnp.bfloat16)


def route_table(key):
    base_key = jax.random.fold_in(key, 53)
    blocks = TOKENS // TOK_DEV
    slot_count = GROUPS * GROUP_CAP
    favored = jax.random.randint(jax.random.fold_in(base_key, 1), (), 0, GROUPS)

    def one_block(block_key):
        slot_order = jax.random.permutation(jax.random.fold_in(block_key, 1), slot_count)
        ranking = jnp.where(slot_order // GROUP_CAP == favored, 0, 1) * slot_count + jnp.arange(slot_count, dtype=jnp.int32)
        taken_slots = slot_order[jnp.argsort(ranking)][:TOK_DEV]
        shuffled = taken_slots[jax.random.permutation(jax.random.fold_in(block_key, 2), TOK_DEV)]
        chosen = shuffled // GROUP_CAP
        first_member = jax.random.randint(jax.random.fold_in(block_key, 3), (TOK_DEV,), 0, GROUP_EXPERTS)
        stepping = jax.random.randint(jax.random.fold_in(block_key, 4), (TOK_DEV,), 1, GROUP_EXPERTS)
        second = (first_member + stepping) % GROUP_EXPERTS
        return (chosen, jnp.stack([first_member, second], axis=1))
    block_keys = jax.random.split(jax.random.fold_in(base_key, 2), blocks)
    chosen, members = jax.vmap(one_block)(block_keys)
    return (chosen.reshape(TOKENS).astype(jnp.int32), members.reshape(TOKENS, TOP).astype(jnp.int32))


def draw_route_group(key, part):
    return route_table(key)[0]


def draw_route_member(key, part):
    return route_table(key)[1]


def block_scale(key, extent, pieces, smallest, top_value):
    def one(axis_at, shards_of):
        draws = jax.random.uniform(jax.random.fold_in(jax.random.fold_in(key, 6), axis_at), (shards_of,), jnp.float32, smallest / len(pieces), top_value / len(pieces))
        return jnp.repeat(jnp.exp(draws), extent[axis_at] // shards_of).reshape((-1,) + (1,) * (len(extent) - axis_at - 1))

    gain = one(*pieces[0])
    for cut in pieces[1:]:
        gain = gain * one(*cut)
    return gain


def noise(stream_key, extent, scale, most, cuts=(), kind=jnp.bfloat16):
    values = jax.random.normal(stream_key, extent, jnp.float32) * scale
    if len(cuts) > 0:
        values = block_scale(stream_key, extent, cuts, -0.22, 0.18) * values
    return jnp.clip(values, min=-most, max=most).astype(kind)


def setup_inputs(seed: int = 0) -> dict:
    arg_keys = jax.random.split(jax.random.key(seed), 15)
    return {
        "queries": draw_queries(jax.random.fold_in(arg_keys[14], 71), 0),
        "key_heads": draw_key_heads(jax.random.fold_in(arg_keys[14], 71), 0),
        "value_heads": noise(arg_keys[2], (TOKENS, KV_HEADS * HEAD_DIM), 1.0, 4.0, ((0, 16),)),
        "sink_logit": jnp.clip(-2.0 + 9.0 * jax.random.uniform(arg_keys[3], (HEADS,), jnp.float32) ** block_scale(arg_keys[3], (HEADS,), ((0, 16),), -0.2, 0.2), -2.0, 7.0),
        "out_weight": noise(arg_keys[4], (HEADS * HEAD_DIM, D), (HEADS * HEAD_DIM) ** -0.5, 0.125, ((0, 16),)),
        "residual": noise(arg_keys[5], (TOKENS, D), 1.0, 6.0, ((0, 256),)),
        "mixer_gain": jnp.clip(1.0 + 0.18 * jax.random.normal(arg_keys[6], (D,), jnp.float32), 0.1, 1.9),
        "expert_gain": jnp.clip(1.0 + 0.18 * jax.random.normal(arg_keys[7], (D,), jnp.float32), 0.1, 1.9),
        "route_group": draw_route_group(jax.random.fold_in(arg_keys[14], 71), 0),
        "route_member": draw_route_member(jax.random.fold_in(arg_keys[14], 71), 0),
        "route_weight": jnp.clip(0.19921875 + 0.80078125 * jax.random.uniform(arg_keys[10], (TOKENS, TOP), jnp.float32) ** block_scale(arg_keys[10], (TOKENS, TOP), ((0, 256),), -0.2, 0.2), 0.19921875, 1.0).astype(jnp.bfloat16),
        "gate_weight": noise(arg_keys[11], (EXPERTS, D, EXP_HID), D ** -0.5, 0.125, ((0, 16), (2, 16))),
        "up_weight": noise(arg_keys[12], (EXPERTS, D, EXP_HID), D ** -0.5, 0.125, ((0, 16), (2, 16))),
        "down_weight": noise(arg_keys[13], (EXPERTS, EXP_HID, D), EXP_HID ** -0.5, 0.125, ((0, 16), (1, 16))),
    }


EPS = 1e-06
NEG_BIG = -1e+30

def head_attention(queries, key_heads, value_heads, sink_logit):
    blocks = TOKENS // BLOCK
    span_rows = BLOCK + 2 * WINDOW
    key_group = HEADS // KV_HEADS
    query_pos = jnp.arange(TOKENS, dtype=jnp.int32).reshape(blocks, BLOCK)
    key_pos = (jnp.arange(blocks, dtype=jnp.int32) * BLOCK)[:, None] + jnp.arange(span_rows, dtype=jnp.int32)[None, :] - WINDOW
    inside = (jnp.abs(query_pos[:, :, None] - key_pos[:, None, :]) <= WINDOW) & (key_pos >= 0)[:, None, :] & (key_pos < TOKENS)[:, None, :]
    gather_at = jnp.clip(key_pos, 0, TOKENS - 1)

    def one_head(head_index):
        query_cols = lax.dynamic_slice_in_dim(queries, head_index * HEAD_DIM, HEAD_DIM, 1).reshape(blocks, BLOCK, HEAD_DIM)
        kv_start = head_index // key_group * HEAD_DIM
        key_cols = lax.dynamic_slice_in_dim(key_heads, kv_start, HEAD_DIM, 1)[gather_at]
        value_cols = lax.dynamic_slice_in_dim(value_heads, kv_start, HEAD_DIM, 1)[gather_at]
        scores = jnp.einsum('nqd,nkd->nqk', query_cols.astype(jnp.float32), key_cols.astype(jnp.float32)) * HEAD_DIM ** (-0.5)
        scores = jnp.where(inside, scores, NEG_BIG)
        sink_value = sink_logit[head_index].astype(jnp.float32)
        row_top = jnp.maximum(lax.optimization_barrier(jnp.max(scores, axis=2, keepdims=True)), sink_value)
        exp_terms = jnp.exp(scores - row_top)
        row_mass = lax.optimization_barrier(jnp.sum(exp_terms, axis=2, keepdims=True)) + jnp.exp(sink_value - row_top)
        weight = (exp_terms / row_mass).astype(jnp.bfloat16)
        result = jnp.einsum('nqk,nkd->nqd', weight.astype(jnp.float32), value_cols.astype(jnp.float32)).astype(jnp.bfloat16)
        return result.reshape(TOKENS, HEAD_DIM)
    per_head = lax.map(one_head, jnp.arange(HEADS, dtype=jnp.int32))
    return jnp.transpose(per_head, (1, 0, 2)).reshape(TOKENS, HEADS * HEAD_DIM)

def merge_heads(attended, out_weight):
    width = HEADS // N_TP * HEAD_DIM

    def add_block(block_index, running):
        columns = lax.dynamic_slice_in_dim(attended, block_index * width, width, 1)
        weight_rows = lax.dynamic_slice_in_dim(out_weight, block_index * width, width, 0)
        product = jnp.dot(columns, weight_rows, preferred_element_type=jnp.float32).astype(jnp.bfloat16)
        product = lax.optimization_barrier(product)
        return running + product.astype(jnp.float32)
    return lax.fori_loop(0, N_TP, add_block, jnp.zeros((TOKENS, D), jnp.float32))

def reference(queries, key_heads, value_heads, sink_logit, out_weight, residual, mixer_gain, expert_gain, route_group, route_member, route_weight, gate_weight, up_weight, down_weight):
    attended = head_attention(queries, key_heads, value_heads, sink_logit)
    projected = merge_heads(attended, out_weight)
    proj_scale = lax.rsqrt(lax.optimization_barrier(jnp.mean(projected * projected, axis=1, keepdims=True)) + EPS)
    mixed_rows = (residual.astype(jnp.float32) + mixer_gain.astype(jnp.float32) * (projected * proj_scale)).astype(jnp.bfloat16)
    mixed_float = mixed_rows.astype(jnp.float32)
    norm_scale = lax.rsqrt(lax.optimization_barrier(jnp.mean(mixed_float * mixed_float, axis=1, keepdims=True)) + EPS)
    normed = (mixed_float * norm_scale * expert_gain.astype(jnp.float32)).astype(jnp.bfloat16)
    blocks = TOKENS // TOK_DEV
    slots = blocks * GROUP_CAP
    grouped = route_group.reshape(blocks, TOK_DEV)
    chosen = (grouped[:, :, None] == jnp.arange(GROUPS, dtype=jnp.int32)[None, None, :]).astype(jnp.int32)
    group_rank = lax.optimization_barrier(jnp.sum(chosen * (jnp.cumsum(chosen, axis=1) - 1), axis=2))
    block_ids = jnp.arange(blocks, dtype=jnp.int32)[:, None]
    dest = (grouped * slots + block_ids * GROUP_CAP + group_rank).reshape(TOKENS).astype(jnp.int32)
    member_ids = jnp.arange(GROUP_EXPERTS, dtype=jnp.int32)
    token_gates = lax.optimization_barrier(jnp.sum(route_weight.astype(jnp.float32)[:, :, None] * (route_member[:, :, None] == member_ids[None, None, :]).astype(jnp.float32), axis=1))
    slot_rows = jnp.zeros((GROUPS * slots, D), jnp.bfloat16).at[dest].set(normed)
    slot_gates = jnp.zeros((GROUPS * slots, GROUP_EXPERTS), jnp.float32).at[dest].set(token_gates)
    hid_dev = EXP_HID // N_TP

    def group_experts(operands):
        rows_in, gates_in, gate_w, up_w, down_w = operands
        gate_pre = jnp.einsum('md,edh->meh', rows_in.astype(jnp.float32), gate_w.astype(jnp.float32))
        up_pre = jnp.einsum('md,edh->meh', rows_in.astype(jnp.float32), up_w.astype(jnp.float32))
        hidden = (jax.nn.silu(gate_pre) * up_pre * gates_in[:, :, None]).astype(jnp.bfloat16)
        hidden = hidden.reshape(slots, GROUP_EXPERTS, N_TP, hid_dev)
        down_blocks = down_w.reshape(GROUP_EXPERTS, N_TP, hid_dev, D)
        parts = jnp.einsum('mejh,ejhd->mjd', hidden.astype(jnp.float32), down_blocks.astype(jnp.float32))
        parts = lax.optimization_barrier(parts.astype(jnp.bfloat16))
        return lax.optimization_barrier(jnp.sum(parts.astype(jnp.float32), axis=1)).astype(jnp.bfloat16)
    group_out = lax.map(group_experts, (slot_rows.reshape(GROUPS, slots, D), slot_gates.reshape(GROUPS, slots, GROUP_EXPERTS), gate_weight.reshape(GROUPS, GROUP_EXPERTS, D, EXP_HID), up_weight.reshape(GROUPS, GROUP_EXPERTS, D, EXP_HID), down_weight.reshape(GROUPS, GROUP_EXPERTS, EXP_HID, D)))
    expert_out = group_out.reshape(GROUPS * slots, D)[dest]
    return (mixed_float + expert_out.astype(jnp.float32)).astype(jnp.bfloat16)
```

```python
import functools

import jax
import jax.numpy as jnp
from jax import lax
from jax.experimental import pallas as pl
from jax.experimental.pallas import tpu as pltpu
from jax.sharding import Mesh
from jax.sharding import PartitionSpec as P

HEADS = 16
KV_HEADS = 4
HEAD_DIM = 128
WINDOW = 128
BLOCK = 128
GROUP_EXPERTS = 3
TP = ("tp_0", "tp_1")
SP_TP = ("sp", "tp_0", "tp_1")


EPS = 1e-06
NEG_BIG = -1e30
VMEM_LIMIT = 60 * 1024 * 1024


def extended(block, sides, width):
    for axis, dim in sides:
        count = lax.axis_size(axis)
        forward = [(i, i + 1) for i in range(count - 1)]
        backward = [(target, source) for source, target in forward]
        low = lax.ppermute(
            lax.slice_in_dim(block, block.shape[dim] - width, None, axis=dim), axis, forward
        )
        high = lax.ppermute(lax.slice_in_dim(block, 0, width, axis=dim), axis, backward)
        block = jnp.concatenate([low, block, high], axis=dim)
    return block


def cut_along(shard, dim, devices):
    dims = shard.shape
    blocks = shard.reshape(*dims[:dim], devices, dims[dim] // devices, *dims[dim + 1 :])
    return jnp.moveaxis(blocks, dim, 0)


def joined_along(blocks, dim):
    dims = list(blocks.shape[1:])
    dims[dim] *= blocks.shape[0]
    return jnp.moveaxis(blocks, 0, dim).reshape(dims)


def exchange_in_order(blocks, axes, order):
    dims = [lax.axis_size(a) for a in axes]
    blocks = blocks.reshape(*dims, *blocks.shape[1:])
    for k in order:
        blocks = lax.all_to_all(blocks, axes[k], split_axis=k, concat_axis=k, tiled=True)
    return blocks.reshape(-1, *blocks.shape[len(axes) :])


def stepwise_exchange(shard, axes, order, split_dim, concat_dim):
    blocks = cut_along(shard, split_dim, lax.axis_size(axes))
    return joined_along(exchange_in_order(blocks, axes, order), concat_dim)


def window_attention(queries, key_heads, value_heads, sink_logit):
    seq_rows = queries.shape[0]
    heads_dev = sink_logit.shape[0]
    key_group = HEADS // KV_HEADS
    key_start = lax.axis_index(TP) * heads_dev // key_group * HEAD_DIM
    key_own = lax.dynamic_slice_in_dim(key_heads, key_start, HEAD_DIM, 1)
    value_own = lax.dynamic_slice_in_dim(value_heads, key_start, HEAD_DIM, 1)
    padded = extended(jnp.stack([key_own, value_own]), (("sp", 1),), WINDOW)
    blocks = seq_rows // BLOCK
    extent = WINDOW // BLOCK
    tile_rows = padded.reshape(2, blocks + 2 * extent, BLOCK, HEAD_DIM)
    key_spans = jnp.concatenate(
        [tile_rows[:, shifted : shifted + blocks] for shifted in range(2 * extent + 1)], axis=2
    )
    offset = lax.axis_index("sp") * seq_rows
    seq_total = seq_rows * lax.axis_size("sp")
    query_pos = offset + jnp.arange(seq_rows, dtype=jnp.int32).reshape(blocks, BLOCK)
    key_pos = (
        offset
        + (jnp.arange(blocks, dtype=jnp.int32) * BLOCK)[:, None]
        + jnp.arange(BLOCK + 2 * WINDOW, dtype=jnp.int32)[None, :]
        - WINDOW
    )
    inside = (
        (jnp.abs(query_pos[:, :, None] - key_pos[:, None, :]) <= WINDOW)
        & (key_pos >= 0)[:, None, :]
        & (key_pos < seq_total)[:, None, :]
    )
    query_blocks = queries.reshape(blocks, BLOCK, heads_dev, HEAD_DIM)
    scores = jnp.einsum(
        "nqhd,nkd->nhqk", query_blocks, key_spans[0], preferred_element_type=jnp.float32
    ) * HEAD_DIM ** (-0.5)
    scores = jnp.where(inside[:, None], scores, NEG_BIG)
    sink_col = sink_logit[None, :, None, None]
    row_top = jnp.maximum(jnp.max(scores, axis=3, keepdims=True), sink_col)
    exp_terms = jnp.exp(scores - row_top)
    row_mass = jnp.sum(exp_terms, axis=3, keepdims=True) + jnp.exp(sink_col - row_top)
    weight = (exp_terms / row_mass).astype(jnp.bfloat16)
    attended = jnp.einsum(
        "nhqk,nkd->nqhd", weight, key_spans[1], preferred_element_type=jnp.float32
    ).astype(jnp.bfloat16)
    return attended.reshape(seq_rows, heads_dev * HEAD_DIM)


MESH_ID = pl.DeviceIdType.MESH
SLOT = 16


def expert_kernel(
    n_sp,
    n_z,
    cap,
    normed,
    mixed,
    placing,
    placing_t,
    gate_rows,
    pick,
    pick_t,
    gate_pick,
    wg,
    wu,
    wd,
    out,
    send,
    arr,
    rows,
    gates,
    gcol,
    hidden,
    w_in,
    w_out,
    own,
    oth,
    got,
    hop,
    ret,
    back,
    w_sem,
    disp_s,
    disp_r,
    ring_s,
    ring_r,
    rgate_s,
    rgate_r,
    pair_s,
    pair_r,
    pgate_s,
    pgate_r,
    sum_s,
    sum_r,
    hop_s,
    hop_r,
    ret_s,
    ret_r,
):
    sp, z, c = lax.axis_index("sp"), lax.axis_index("tp_0"), lax.axis_index("tp_1")
    width = normed.shape[1]
    experts, hid = wd.shape[0], wd.shape[1]
    half = n_sp // 2
    hr = half * cap
    far = n_z // 2
    tile = 256 if width % 256 == 0 else width
    sends = []

    def push(src, dst, s_sem, r_sem, dev):
        copy = pltpu.make_async_remote_copy(
            src_ref=src, dst_ref=dst, send_sem=s_sem, recv_sem=r_sem, device_id=dev, device_id_type=MESH_ID
        )
        copy.start()
        sends.append(copy)
        return copy

    partner = (sp, z, 1 - c)
    ring_dev = ((sp, lax.rem(z + 1, n_z), c), (sp, lax.rem(z + n_z - 1, n_z), c))

    loads = []
    for e in range(experts):
        loads.append(pltpu.make_async_copy(wg.at[e], w_in.at[e, :, pl.ds(0, hid)], w_sem.at[e, 0]))
        loads.append(pltpu.make_async_copy(wu.at[e], w_in.at[e, :, pl.ds(hid, hid)], w_sem.at[e, 1]))
        loads.append(pltpu.make_async_copy(wd.at[e], w_out.at[pl.ds(e * hid, hid), :], w_sem.at[e, 2]))
    for load in loads:
        load.start()

    barrier = pltpu.get_barrier_semaphore()
    for j in range(1, n_sp):
        pl.semaphore_signal(barrier, inc=1, device_id=(lax.rem(sp + j, n_sp), z, c), device_id_type=MESH_ID)
    for dev in ring_dev + (partner,):
        pl.semaphore_signal(barrier, inc=1, device_id=dev, device_id_type=MESH_ID)

    head = jnp.dot(placing[...], normed[:, 0:128], preferred_element_type=jnp.float32)
    send[:, 0:128] = (head + gate_rows[...].astype(jnp.float32)).astype(jnp.bfloat16)
    send[:, 128:] = jnp.dot(placing[...], normed[:, 128:], preferred_element_type=jnp.float32).astype(
        jnp.bfloat16
    )
    pl.semaphore_wait(barrier, n_sp - 1 + 3)

    disp = [None]
    for j in range(1, n_sp):
        block = pl.ds(j * SLOT, SLOT)
        disp.append(
            push(send.at[block], arr.at[block], disp_s.at[j], disp_r.at[j], (lax.rem(sp + j, n_sp), z, c))
        )
    arr[0:SLOT] = send[0:SLOT]

    def reach(dr, hf):
        return far if dr == hf else far - 1

    def at(dr, d):
        return (n_z - d) % n_z if dr == 0 else d

    def part(rc, hf):
        return pl.ds((rc * 2 + hf) * hr, hr)

    ring = {}
    ring_g = {}
    pair = {}

    def ring_send(dr, d, hf):
        src, dst = at(dr, d), at(dr, d + 1)
        sem = (dr, d, hf)
        ring[sem] = push(
            rows.at[src, part(0, hf)], rows.at[dst, part(0, hf)], ring_s.at[sem], ring_r.at[sem], ring_dev[dr]
        )
        ring_g[sem] = push(
            gates.at[src, 0, hf], gates.at[dst, 0, hf], rgate_s.at[sem], rgate_r.at[sem], ring_dev[dr]
        )

    def ring_wait(dr, d, hf):
        ring[(dr, d - 1, hf)].wait_recv()
        ring_g[(dr, d - 1, hf)].wait_recv()

    def pair_send(o, hf):
        pair[(o, hf)] = (
            push(rows.at[o, part(0, hf)], rows.at[o, part(1, hf)], pair_s.at[o, hf], pair_r.at[o, hf], partner),
            push(gates.at[o, 0, hf], gates.at[o, 1, hf], pgate_s.at[o, hf], pgate_r.at[o, hf], partner),
        )

    for hf in range(2):
        for j in range(hf * half, (hf + 1) * half):
            if j > 0:
                disp[j].wait_recv()
        block = pl.ds(hf * half * SLOT, half * SLOT)
        rows[0, part(0, hf)] = jnp.dot(pick[...], arr[block, :], preferred_element_type=jnp.float32).astype(
            jnp.bfloat16
        )
        gates[0, 0, hf] = jnp.dot(
            gate_pick[...], arr[block, 0:128], preferred_element_type=jnp.float32
        ).astype(jnp.bfloat16)
        ring_send(0, 0, hf)
        ring_send(1, 0, hf)
        pair_send(0, hf)

    for load in loads:
        load.wait()

    eye = jnp.where(
        lax.broadcasted_iota(jnp.int32, (hr, 128), 0) == lax.broadcasted_iota(jnp.int32, (hr, 128), 1), 1.0, 0.0
    ).astype(jnp.bfloat16)
    summed = {}

    def compute(o):
        for hf in range(2):
            for copy in pair[(o, hf)]:
                copy.wait_recv()
        for rc in range(2):
            for hf in range(2):
                gcol[part(rc, hf)] = lax.dot_general(
                    eye, gates[o, rc, hf], (((1,), (1,)), ((), ())), preferred_element_type=jnp.float32
                )
        for e in range(experts):
            pre = jnp.dot(rows[o], w_in[e], preferred_element_type=jnp.float32)
            gate_pre, up_pre = pre[:, :hid], pre[:, hid:]
            scaled = gate_pre / (1.0 + jnp.exp(-gate_pre)) * up_pre * gcol[:, e : e + 1]
            hidden[:, e * hid : (e + 1) * hid] = scaled.astype(jnp.bfloat16)

        def down(i, carry):
            columns = pl.ds(pl.multiple_of(i * tile, tile), tile)
            piece = jnp.dot(hidden[...], w_out[:, columns], preferred_element_type=jnp.float32).astype(
                jnp.bfloat16
            )
            own[o, :, columns] = piece[: 2 * hr]
            oth[o, :, columns] = piece[2 * hr :]
            return carry

        lax.fori_loop(0, width // tile, down, 0)
        summed[o] = push(oth.at[o], got.at[o], sum_s.at[o], sum_r.at[o], partner)

    hops = {}
    settled = set()

    def settle(o):
        if o not in settled:
            summed[o].wait_recv()
            settled.add(o)

    def half_rows(hf, i):
        return pl.ds(pl.multiple_of(hf * hr + i * 16, 16), 16)

    def hop_send(dr, d, hf):
        o = (n_z - d) % n_z if dr == 1 else d
        settle(o)
        start = d == reach(dr, hf)
        if start:
            src = own.at[o, pl.ds(hf * hr, hr)]
        else:
            hops[(dr, d + 1, hf)].wait_recv()
            src = hop.at[dr, d, hf]

        def add(i, carry):
            local = pl.ds(pl.multiple_of(i * 16, 16), 16)
            total = own[o, half_rows(hf, i)].astype(jnp.float32) + got[o, half_rows(hf, i)].astype(jnp.float32)
            if not start:
                total = total + hop[dr, d, hf, local].astype(jnp.float32)
            src[local] = total.astype(jnp.bfloat16)
            return carry

        lax.fori_loop(0, hr // 16, add, 0)
        sem = (dr, d, hf)
        hops[sem] = push(src, hop.at[dr, d - 1, hf], hop_s.at[sem], hop_r.at[sem], ring_dev[dr])

    compute(0)
    order = []
    for d in range(1, far):
        order += [(d, 0), (d, 1)]
    for d, sub in order:
        for dr in range(2):
            hf = sub
            ring_wait(dr, d, hf)
            if d < reach(dr, hf):
                ring_send(dr, d, hf)
            pair_send(at(dr, d), hf)
        if sub == 1:
            compute(at(0, d))
            compute(at(1, d))
    for dr in range(2):
        hop_send(dr, far - 1, 1 - dr)
    for dr in range(2):
        ring_wait(dr, far, dr)
        pair_send(at(dr, far), dr)
    compute(far)
    for dr in range(2):
        hop_send(dr, far, dr)
    for d in range(far - 2, 0, -1):
        for dr in range(2):
            hop_send(dr, d, 1 - dr)
        for dr in range(2):
            hop_send(dr, d + 1, dr)
    for dr in range(2):
        hop_send(dr, 1, dr)

    settle(0)
    returned = [None] * n_sp
    for hf in range(2):
        for dr in range(2):
            hops[(dr, 1, hf)].wait_recv()

        def finish(i, carry):
            local = pl.ds(pl.multiple_of(i * 16, 16), 16)
            total = own[0, half_rows(hf, i)].astype(jnp.float32) + got[0, half_rows(hf, i)].astype(jnp.float32)
            total = total + (hop[0, 0, hf, local].astype(jnp.float32) + hop[1, 0, hf, local].astype(jnp.float32))
            own[0, half_rows(hf, i)] = total.astype(jnp.bfloat16)
            return carry

        lax.fori_loop(0, hr // 16, finish, 0)
        ret[pl.ds(hf * half * SLOT, half * SLOT)] = jnp.dot(
            pick_t[...], own[0, pl.ds(hf * hr, hr)], preferred_element_type=jnp.float32
        ).astype(jnp.bfloat16)
        for j in range(hf * half, (hf + 1) * half):
            block = pl.ds(j * SLOT, SLOT)
            if j == 0:
                back[block] = ret[block]
            else:
                returned[j] = push(
                    ret.at[block], back.at[block], ret_s.at[j], ret_r.at[j], (lax.rem(sp + n_sp - j, n_sp), z, c)
                )
    for j in range(1, n_sp):
        returned[j].wait_recv()
    expert_out = jnp.dot(placing_t[...], back[...], preferred_element_type=jnp.float32)
    out[...] = (mixed[...].astype(jnp.float32) + expert_out).astype(jnp.bfloat16)
    for copy in sends:
        copy.wait_send()


def routed_experts(normed, mixed, route_group, token_gates, wg, wu, wd, cap):
    n_sp, n_z = lax.axis_size("sp"), lax.axis_size("tp_0")
    tok_rows, width = normed.shape
    experts, hid = wd.shape[0], wd.shape[1]
    half = n_sp // 2
    hr = half * cap
    far = n_z // 2
    group_ids = jnp.arange(n_sp, dtype=jnp.int32)
    chosen = (route_group[:, None] == group_ids[None, :]).astype(jnp.int32)
    rank = jnp.sum(chosen * (jnp.cumsum(chosen, axis=0) - 1), axis=1)
    ahead = jnp.mod(route_group - lax.axis_index("sp"), n_sp)
    slot = ahead * SLOT + rank
    slots = jnp.arange(n_sp * SLOT, dtype=jnp.int32)
    placing = (slots[:, None] == slot[None, :]).astype(jnp.bfloat16)
    placing_t = (slot[:, None] == slots[None, :]).astype(jnp.bfloat16)
    lane = jnp.mod(ahead, half) * cap + rank
    lane_hot = (lane[:, None] == jnp.arange(128, dtype=jnp.int32)[None, :]).astype(jnp.float32)
    members = jnp.arange(experts, dtype=jnp.int32)
    row_at = (ahead * SLOT + cap)[None, :] + members[:, None]
    row_hot = (slots[:, None, None] == row_at[None]).astype(jnp.bfloat16).reshape(n_sp * SLOT, -1)
    lane_val = (token_gates.astype(jnp.float32).T[:, :, None] * lane_hot[None]).astype(jnp.bfloat16)
    gate_rows = jnp.dot(row_hot, lane_val.reshape(-1, 128), preferred_element_type=jnp.float32).astype(
        jnp.bfloat16
    )
    r = jnp.arange(hr, dtype=jnp.int32)
    padded = r // cap * SLOT + r % cap
    i = jnp.arange(half * SLOT, dtype=jnp.int32)
    pick = (i[None, :] == padded[:, None]).astype(jnp.bfloat16)
    pick_t = (i[:, None] == padded[None, :]).astype(jnp.bfloat16)
    gate_pick = (
        (i[None, :] % SLOT == jnp.arange(16, dtype=jnp.int32)[:, None] + cap) & (jnp.arange(16)[:, None] < experts)
    ).astype(jnp.bfloat16)
    bf = jnp.bfloat16
    vmem = pl.BlockSpec(memory_space=pltpu.VMEM)
    anywhere = pl.BlockSpec(memory_space=pl.ANY)
    dma = pltpu.SemaphoreType.DMA
    return pl.pallas_call(
        functools.partial(expert_kernel, n_sp, n_z, cap),
        out_shape=jax.ShapeDtypeStruct((tok_rows, width), bf),
        in_specs=[vmem] * 8 + [anywhere] * 3,
        out_specs=vmem,
        scratch_shapes=[
            pltpu.VMEM((n_sp * SLOT, width), bf),
            pltpu.VMEM((n_sp * SLOT, width), bf),
            pltpu.VMEM((n_z, 4 * hr, width), bf),
            pltpu.VMEM((n_z, 2, 2, 16, 128), bf),
            pltpu.VMEM((4 * hr, 16), jnp.float32),
            pltpu.VMEM((4 * hr, experts * hid), bf),
            pltpu.VMEM((experts, width, 2 * hid), bf),
            pltpu.VMEM((experts * hid, width), bf),
            pltpu.VMEM((n_z, 2 * hr, width), bf),
            pltpu.VMEM((n_z, 2 * hr, width), bf),
            pltpu.VMEM((n_z, 2 * hr, width), bf),
            pltpu.VMEM((2, far, 2, hr, width), bf),
            pltpu.VMEM((n_sp * SLOT, width), bf),
            pltpu.VMEM((n_sp * SLOT, width), bf),
            dma((experts, 3)),
            dma((n_sp,)),
            dma((n_sp,)),
            dma((2, far, 2)),
            dma((2, far, 2)),
            dma((2, far, 2)),
            dma((2, far, 2)),
            dma((n_z, 2)),
            dma((n_z, 2)),
            dma((n_z, 2)),
            dma((n_z, 2)),
            dma((n_z,)),
            dma((n_z,)),
            dma((2, far + 1, 2)),
            dma((2, far + 1, 2)),
            dma((n_sp,)),
            dma((n_sp,)),
        ],
        compiler_params=pltpu.CompilerParams(
            collective_id=1, has_side_effects=True, vmem_limit_bytes=VMEM_LIMIT
        ),
    )(normed, mixed, placing, placing_t, gate_rows, pick, pick_t, gate_pick, wg, wu, wd)


def per_device(
    queries,
    key_heads,
    value_heads,
    sink_logit,
    out_weight,
    residual,
    mixer_gain,
    expert_gain,
    route_group,
    route_member,
    route_weight,
    gate_weight,
    up_weight,
    down_weight,
):
    attended = window_attention(queries, key_heads, value_heads, sink_logit)
    tok_rows = residual.shape[0]
    width = out_weight.shape[1]
    by_token = stepwise_exchange(attended, TP, (1, 0), 0, 1)
    shard_rows = out_weight.shape[0]
    weight_piece = lax.all_gather(out_weight, TP, axis=0, tiled=True)
    shards = weight_piece.shape[0] // shard_rows
    columns = by_token
    columns = columns.reshape(tok_rows, shards, shard_rows)
    weight_slabs = weight_piece.reshape(shards, shard_rows, width)
    products = jnp.einsum("rkc,kcd->krd", columns, weight_slabs, preferred_element_type=jnp.float32)
    rounded = lax.optimization_barrier(products.astype(jnp.bfloat16))
    projected = jnp.sum(rounded.astype(jnp.float32), axis=0)
    proj_scale = lax.rsqrt(jnp.mean(projected * projected, axis=1, keepdims=True) + EPS)
    mixed_rows = (residual.astype(jnp.float32) + mixer_gain * (projected * proj_scale)).astype(
        jnp.bfloat16
    )
    mixed_float = mixed_rows.astype(jnp.float32)
    norm_scale = lax.rsqrt(jnp.mean(mixed_float * mixed_float, axis=1, keepdims=True) + EPS)
    normed = (mixed_float * norm_scale * expert_gain).astype(jnp.bfloat16)
    groups = lax.axis_size("sp")
    capacity = max(2, (5 * tok_rows + 4 * groups - 1) // (4 * groups))
    member_ids = jnp.arange(GROUP_EXPERTS, dtype=jnp.int32)
    token_gates = jnp.sum(
        route_weight.astype(jnp.float32)[:, :, None]
        * (route_member[:, :, None] == member_ids[None, None, :]).astype(jnp.float32),
        axis=1,
    )
    return routed_experts(
        normed, mixed_rows, route_group, token_gates, gate_weight, up_weight, down_weight, capacity
    )


def solution(mesh):
    torus = Mesh(mesh.devices.reshape(mesh.shape["sp"], 8, 2), ("sp", "tp_0", "tp_1"))
    placed = (
        P("sp", TP),
        P("sp", None),
        P("sp", None),
        P(TP),
        P(TP, None),
        P(SP_TP, None),
        P(),
        P(),
        P(SP_TP),
        P(SP_TP, None),
        P(SP_TP, None),
        P("sp", None, TP),
        P("sp", None, TP),
        P("sp", TP, None),
    )
    return jax.shard_map(
        per_device, mesh=torus, in_specs=placed, out_specs=P(SP_TP, None), check_vma=False
    )
```

```python
import functools

import jax
import jax.numpy as jnp
import numpy as np
from jax import lax
from jax.experimental import pallas as pl
from jax.experimental.pallas import tpu as pltpu
from jax.sharding import Mesh
from jax.sharding import PartitionSpec as P

HEADS = 16
KV_HEADS = 4
HEAD_DIM = 128
WINDOW = 128
BLOCK = 128
GROUP_EXPERTS = 3
GROUP_CAP = 10
SLOT = 16
TP = ("tp_0", "tp_1")
SP_TP = ("sp", "tp_0", "tp_1")
MESH_ID = pl.DeviceIdType.MESH
VMEM_LIMIT = 62 * 1024 * 1024

EPS = 1e-06
NEG_BIG = -1e30
BF = jnp.bfloat16
F32 = jnp.float32


def one_hot(condition):
    return jnp.where(condition, 1.0, 0.0).astype(BF)


def iota(shape, dim):
    return lax.broadcasted_iota(jnp.int32, shape, dim)


def layer_kernel(
    n_sp,
    n_x,
    n_z,
    kv_share,
    cap,
    queries,
    key_heads,
    value_heads,
    sink,
    out_weight,
    residual,
    mixer_gain,
    expert_gain,
    info,
    pick,
    pick_t,
    gate_pick,
    wg,
    wu,
    wd,
    out,
    q_buf,
    k_buf,
    v_buf,
    att,
    by_token,
    w_proj,
    proj,
    normed,
    mixed,
    placing,
    gate_rows,
    send,
    arr,
    rows,
    gates,
    gcol,
    hidden,
    w_in,
    w_out,
    own,
    oth,
    got,
    hop,
    ret,
    back,
    load_sem,
    halo_s,
    halo_r,
    a2a_s,
    a2a_r,
    col_s,
    col_r,
    near_s,
    near_r,
    wide_s,
    wide_r,
    wpair_s,
    wpair_r,
    w_sem,
    disp_s,
    disp_r,
    ring_s,
    ring_r,
    rgate_s,
    rgate_r,
    pair_s,
    pair_r,
    pgate_s,
    pgate_r,
    sum_s,
    sum_r,
    hop_s,
    hop_r,
    ret_s,
    ret_r,
):
    sp, z, c = lax.axis_index("sp"), lax.axis_index("tp_0"), lax.axis_index("tp_1")
    me = z * 2 + c
    n_tp = 2 * n_z
    y, x = lax.div(sp, n_x), lax.rem(sp, n_x)
    n_y = n_sp // n_x
    tok, width = residual.shape
    experts, hid = wd.shape[0], wd.shape[1]
    half = n_sp // 2
    hr = half * cap
    far = n_z // 2
    tile = 256
    sends = []

    def remote(src, dst, s_sem, r_sem, dev):
        return pltpu.make_async_remote_copy(
            src_ref=src, dst_ref=dst, send_sem=s_sem, recv_sem=r_sem, device_id=dev, device_id_type=MESH_ID
        )

    def push(src, dst, s_sem, r_sem, dev):
        copy = remote(src, dst, s_sem, r_sem, dev)
        copy.start()
        sends.append(copy)
        return copy

    partner = (sp, z, 1 - c)
    ring_dev = ((sp, lax.rem(z + 1, n_z), c), (sp, lax.rem(z + n_z - 1, n_z), c))

    seq = q_buf.shape[0]
    head_at = pl.ds(pl.multiple_of(lax.div(me, kv_share) * HEAD_DIM, HEAD_DIM), HEAD_DIM)
    inner = pl.ds(WINDOW, seq)
    col_own = pl.ds(pl.multiple_of(sp * 128, 128), 128)
    lanes_own = pl.ds(pl.multiple_of(lax.rem(x, 2) * 128, 128), 128)
    w_own = w_proj.at[y, lax.div(x, 2), z, c, :, lanes_own]
    first = [
        pltpu.make_async_copy(key_heads.at[:, head_at], k_buf.at[inner], load_sem.at[0]),
        pltpu.make_async_copy(value_heads.at[:, head_at], v_buf.at[inner], load_sem.at[1]),
        pltpu.make_async_copy(out_weight.at[:, col_own], w_own, load_sem.at[2]),
        pltpu.make_async_copy(queries, q_buf, load_sem.at[3]),
    ]
    for load in first:
        load.start()
    loads = []
    for e in range(experts):
        loads.append(pltpu.make_async_copy(wg.at[e], w_in.at[e, :, pl.ds(0, hid)], w_sem.at[e, 0]))
        loads.append(pltpu.make_async_copy(wu.at[e], w_in.at[e, :, pl.ds(hid, hid)], w_sem.at[e, 1]))
        loads.append(pltpu.make_async_copy(wd.at[e], w_out.at[pl.ds(e * hid, hid), :], w_sem.at[e, 2]))

    barrier = pltpu.get_barrier_semaphore()
    for j in range(1, n_sp):
        pl.semaphore_signal(barrier, inc=1, device_id=(lax.rem(sp + j, n_sp), z, c), device_id_type=MESH_ID)
    for j in range(1, n_tp):
        n = lax.rem(me + j, n_tp)
        pl.semaphore_signal(
            barrier, inc=1, device_id=(sp, lax.div(n, 2), lax.rem(n, 2)), device_id_type=MESH_ID
        )
    for load in first:
        load.wait()
    pl.semaphore_wait(barrier, n_sp - 1 + n_tp - 1)

    after, before = lax.rem(sp + 1, n_sp), lax.rem(sp + n_sp - 1, n_sp)
    low, high = pl.ds(0, WINDOW), pl.ds(WINDOW + seq, WINDOW)
    halo = []
    for i, buf in enumerate((k_buf, v_buf)):
        halo.append(push(buf.at[pl.ds(seq, WINDOW)], buf.at[low], halo_s.at[0, i], halo_r.at[0, i], (after, z, c)))
        halo.append(push(buf.at[pl.ds(WINDOW, WINDOW)], buf.at[high], halo_s.at[1, i], halo_r.at[1, i], (before, z, c)))

    def col_region(d):
        return w_proj.at[y, lax.div(x, 2), lax.rem(z + n_z - d, n_z), c, :, lanes_own]

    column = []
    for k in range(1, n_z):
        d = (k + 1) // 2 if k % 2 else n_z - k // 2
        push(w_own, w_own, col_s.at[d], col_r.at[d], (sp, lax.rem(z + d, n_z), c))
        column.append(d)
    for load in loads:
        load.start()

    sink_val = sink[0, 0]
    q_pos = iota((BLOCK, BLOCK + 2 * WINDOW), 0)
    k_pos = iota((BLOCK, BLOCK + 2 * WINDOW), 1)

    def attend(n):
        @pl.when(n == 0)
        def _():
            for i in range(2):
                halo[2 * i].wait_recv()

        @pl.when(n == n_tp - 1)
        def _():
            for i in range(2):
                halo[2 * i + 1].wait_recv()

        start = pl.multiple_of(n * BLOCK, BLOCK)
        keys = pl.ds(start, BLOCK + 2 * WINDOW)
        scores = lax.dot_general(
            q_buf[pl.ds(start, BLOCK), :], k_buf[keys, :], (((1,), (1,)), ((), ())), preferred_element_type=F32
        ) * HEAD_DIM ** (-0.5)
        lo = jnp.where((sp == 0) & (n == 0), WINDOW, 0)
        hi = jnp.where((sp == n_sp - 1) & (n == n_tp - 1), BLOCK + WINDOW, BLOCK + 2 * WINDOW)
        inside = (k_pos >= q_pos) & (k_pos <= q_pos + 2 * WINDOW) & (k_pos >= lo) & (k_pos < hi)
        scores = jnp.where(inside, scores, NEG_BIG)
        top = jnp.maximum(jnp.max(scores, axis=1, keepdims=True), sink_val)
        terms = jnp.exp(scores - top)
        mass = jnp.sum(terms, axis=1, keepdims=True) + jnp.exp(sink_val - top)
        value = jnp.dot(terms.astype(BF), v_buf[keys, :], preferred_element_type=F32)
        return (value / mass).astype(BF)

    my_cols = pl.ds(pl.multiple_of(me * HEAD_DIM, HEAD_DIM), HEAD_DIM)

    def a2a_copy(t, n):
        return remote(
            att.at[n], by_token.at[:, my_cols], a2a_s.at[t], a2a_r.at[t], (sp, lax.div(n, 2), lax.rem(n, 2))
        )

    def attend_pair(t, carry):
        ahead, behind = lax.rem(me + t, n_tp), lax.rem(me + n_tp - t, n_tp)
        first_val, second_val = attend(ahead), attend(behind)
        att[ahead] = first_val
        att[behind] = second_val
        a2a_copy(t, ahead).start()
        a2a_copy(n_tp - t, behind).start()
        return carry

    axis_len = (n_x, n_y)
    place = (x, y)
    zq = n_z // 4

    def plane_dev(axis, step):
        at_axis = lax.rem(place[axis] + step + axis_len[axis], axis_len[axis])
        return (y * n_x + at_axis, z, c) if axis == 0 else (at_axis * n_x + x, z, c)

    def plane_region(order, wide, d, dr, hf):
        axis = order if not wide else 1 - order
        at_axis = lax.rem(place[axis] + (axis_len[axis] - d if dr == 0 else d), axis_len[axis])
        zr = pl.ds(order * 2 * zq + hf * zq, zq)
        if wide:
            if axis == 1:
                return w_proj.at[at_axis, :, zr, c]
            lanes = pl.ds(pl.multiple_of(lax.rem(at_axis, 2) * 128, 128), 128)
            return w_proj.at[:, lax.div(at_axis, 2), zr, c, :, lanes]
        if axis == 0:
            lanes = pl.ds(pl.multiple_of(lax.rem(at_axis, 2) * 128, 128), 128)
            return w_proj.at[y, lax.div(at_axis, 2), zr, c, :, lanes]
        return w_proj.at[at_axis, lax.div(x, 2), zr, c, :, lanes_own]

    def plane_reach(order, wide, dr, hf):
        axis = order if not wide else 1 - order
        limit = axis_len[axis] // 2
        return limit if dr == hf else limit - 1

    def plane_copy(order, wide, d, dr, hf):
        axis = order if not wide else 1 - order
        region = plane_region(order, wide, d, dr, hf)
        s_sem, r_sem = (wide_s, wide_r) if wide else (near_s, near_r)
        sem = (order, dr, d, hf)
        return remote(region, region, s_sem.at[sem], r_sem.at[sem], plane_dev(axis, 1 if dr == 0 else -1))

    def plane_send(order, wide, d, dr, hf):
        if d < plane_reach(order, wide, dr, hf):
            copy = plane_copy(order, wide, d, dr, hf)
            copy.start()
            sends.append(copy)

    def plane_wait(order, wide, d, dr, hf):
        axis = order if not wide else 1 - order
        region = plane_region(order, wide, d, dr, hf)
        s_sem, r_sem = (wide_s, wide_r) if wide else (near_s, near_r)
        sem = (order, dr, d - 1, hf)
        remote(region, region, s_sem.at[sem], r_sem.at[sem], plane_dev(axis, 1 if dr == 0 else -1)).wait_recv()

    def plane_steps(order, wide):
        limit = axis_len[order if not wide else 1 - order] // 2
        steps = []
        for d in range(1, limit + 1):
            for sub in range(2):
                for dr in range(2):
                    hf = dr if sub == 0 else 1 - dr
                    if d <= plane_reach(order, wide, dr, hf):
                        steps.append((d, dr, hf))
        return steps

    wpairs = []

    def wpair_send(region, index):
        wpairs.append(push(region, region, wpair_s.at[index], wpair_r.at[index], partner))

    def wpair_wait(order, d, dr, hf, index):
        axis = 1 - order
        at_axis = lax.rem(place[axis] + (axis_len[axis] - d if dr == 0 else d), axis_len[axis])
        zr = pl.ds(order * 2 * zq + hf * zq, zq)
        if axis == 1:
            region = w_proj.at[at_axis, :, zr, 1 - c]
        else:
            lanes = pl.ds(pl.multiple_of(lax.rem(at_axis, 2) * 128, 128), 128)
            region = w_proj.at[:, lax.div(at_axis, 2), zr, 1 - c, :, lanes]
        remote(region, region, wpair_s.at[index], wpair_r.at[index], partner).wait_recv()

    split = max(1, (n_tp // 2) // 2)
    lax.fori_loop(1, 1 + split, attend_pair, 0)
    for d in column:
        remote(w_own, col_region(d), col_s.at[d], col_r.at[d], ring_dev[0]).wait_recv()
    for hf_step in range(2):
        for order in range(2):
            for dr in range(2):
                plane_send(order, False, 0, dr, dr if hf_step == 0 else 1 - dr)
    lax.fori_loop(1 + split, n_tp // 2, attend_pair, 0)
    opposite = lax.rem(me + n_tp // 2, n_tp)
    first_val, own_val = attend(opposite), attend(me)
    att[opposite] = first_val
    by_token[:, my_cols] = own_val
    a2a_copy(n_tp // 2, opposite).start()

    for step in plane_steps(0, False):
        for order in range(2):
            d, dr, hf = step
            plane_wait(order, False, d, dr, hf)
            plane_send(order, False, d, dr, hf)
    for hf_step in range(2):
        for order in range(2):
            for dr in range(2):
                plane_send(order, True, 0, dr, dr if hf_step == 0 else 1 - dr)
    for order in range(2):
        for hf in range(2):
            wpair_send(plane_region(order, True, 0, 0, hf), (order, hf, 0))

    group = info[0:1, :].astype(jnp.int32)
    ahead = group - sp
    ahead = jnp.where(ahead < 0, ahead + n_sp, ahead)
    chosen = iota((n_sp, tok), 0) == ahead
    earlier = one_hot(iota((tok, tok), 0) < iota((tok, tok), 1))
    ranks = jnp.dot(one_hot(chosen), earlier, preferred_element_type=F32)
    rank = jnp.sum(jnp.where(chosen, ranks, 0.0), axis=0, keepdims=True).astype(jnp.int32)
    slot_row = iota((n_sp * SLOT, tok), 0)
    placing[...] = one_hot(slot_row == ahead * SLOT + rank)
    in_half = jnp.where(ahead >= half, ahead - half, ahead)
    lane_hot = one_hot(iota((128, tok), 0) == in_half * cap + rank)
    gate_at = jnp.zeros((n_sp * SLOT, tok), F32)
    for k in range(2):
        member = info[1 + k : 2 + k, :].astype(jnp.int32)
        gate_at = gate_at + jnp.where(slot_row == ahead * SLOT + cap + member, info[3 + k : 4 + k, :], 0.0)
    gate_rows[...] = lax.dot_general(
        gate_at.astype(BF), lane_hot, (((1,), (1,)), ((), ())), preferred_element_type=F32
    )

    for step in plane_steps(0, True):
        for order in range(2):
            d, dr, hf = step
            plane_wait(order, True, d, dr, hf)
            plane_send(order, True, d, dr, hf)
            index = (order, hf, 1 + (d - 1) * 2 + dr)
            wpair_send(plane_region(order, True, d, dr, hf), index)
    for t in range(1, n_tp):
        source = pl.ds(pl.multiple_of(lax.rem(me + n_tp - t, n_tp) * HEAD_DIM, HEAD_DIM), HEAD_DIM)
        remote(att.at[0], by_token.at[:, source], a2a_s.at[t], a2a_r.at[t], partner).wait_recv()
    for order in range(2):
        for hf in range(2):
            wpair_wait(order, 0, 0, hf, (order, hf, 0))
    for d, dr, hf in plane_steps(0, True):
        for order in range(2):
            wpair_wait(order, d, dr, hf, (order, hf, 1 + (d - 1) * 2 + dr))

    w_tiles = width // tile

    def project(i, carry):
        block = w_proj[lax.div(i, w_tiles // n_y), lax.rem(i, w_tiles // n_y)].reshape(n_tp * HEAD_DIM, tile)
        columns = pl.ds(pl.multiple_of(i * tile, tile), tile)
        proj[:, columns] = jnp.dot(by_token[...], block, preferred_element_type=F32)
        return carry

    lax.fori_loop(0, w_tiles, project, 0)

    def norms(i, carry):
        at_rows = pl.ds(pl.multiple_of(i * 16, 16), 16)
        value = proj[at_rows, :]
        scale = lax.rsqrt(jnp.mean(value * value, axis=1, keepdims=True) + EPS)
        mixed_bf = (residual[at_rows, :].astype(F32) + mixer_gain[...] * (value * scale)).astype(BF)
        mixed[at_rows, :] = mixed_bf
        mixed_f = mixed_bf.astype(F32)
        scale = lax.rsqrt(jnp.mean(mixed_f * mixed_f, axis=1, keepdims=True) + EPS)
        normed[at_rows, :] = (mixed_f * scale * expert_gain[...]).astype(BF)
        return carry

    lax.fori_loop(0, tok // 16, norms, 0)

    head = jnp.dot(placing[...], normed[:, 0:128], preferred_element_type=F32)
    send[:, 0:128] = (head + gate_rows[...]).astype(BF)
    send[:, 128:] = jnp.dot(placing[...], normed[:, 128:], preferred_element_type=F32).astype(BF)
    disp = [None]
    for j in range(1, n_sp):
        block = pl.ds(j * SLOT, SLOT)
        disp.append(
            push(send.at[block], arr.at[block], disp_s.at[j], disp_r.at[j], (lax.rem(sp + j, n_sp), z, c))
        )
    arr[0:SLOT] = send[0:SLOT]

    def reach(dr, hf):
        return far if dr == hf else far - 1

    def at(dr, d):
        return (n_z - d) % n_z if dr == 0 else d

    def part(rc, hf):
        return pl.ds((rc * 2 + hf) * hr, hr)

    ring = {}
    ring_g = {}
    pair = {}

    def ring_send(dr, d, hf):
        src, dst = at(dr, d), at(dr, d + 1)
        sem = (dr, d, hf)
        ring[sem] = push(
            rows.at[src, part(0, hf)], rows.at[dst, part(0, hf)], ring_s.at[sem], ring_r.at[sem], ring_dev[dr]
        )
        ring_g[sem] = push(
            gates.at[src, 0, hf], gates.at[dst, 0, hf], rgate_s.at[sem], rgate_r.at[sem], ring_dev[dr]
        )

    def ring_wait(dr, d, hf):
        ring[(dr, d - 1, hf)].wait_recv()
        ring_g[(dr, d - 1, hf)].wait_recv()

    def pair_send(o, hf):
        pair[(o, hf)] = (
            push(rows.at[o, part(0, hf)], rows.at[o, part(1, hf)], pair_s.at[o, hf], pair_r.at[o, hf], partner),
            push(gates.at[o, 0, hf], gates.at[o, 1, hf], pgate_s.at[o, hf], pgate_r.at[o, hf], partner),
        )

    for hf in range(2):
        for j in range(hf * half, (hf + 1) * half):
            if j > 0:
                disp[j].wait_recv()
        block = pl.ds(hf * half * SLOT, half * SLOT)
        rows[0, part(0, hf)] = jnp.dot(pick[...], arr[block, :], preferred_element_type=F32).astype(BF)
        gates[0, 0, hf] = jnp.dot(
            gate_pick[...], arr[block, 0:128], preferred_element_type=F32
        ).astype(BF)
        ring_send(0, 0, hf)
        ring_send(1, 0, hf)
        pair_send(0, hf)

    for load in loads:
        load.wait()

    eye = one_hot(iota((hr, 128), 0) == iota((hr, 128), 1))
    summed = {}

    def compute(o):
        for hf in range(2):
            for copy in pair[(o, hf)]:
                copy.wait_recv()
        for rc in range(2):
            for hf in range(2):
                gcol[part(rc, hf)] = lax.dot_general(
                    eye, gates[o, rc, hf], (((1,), (1,)), ((), ())), preferred_element_type=F32
                )
        for e in range(experts):
            pre = jnp.dot(rows[o], w_in[e], preferred_element_type=F32)
            gate_pre, up_pre = pre[:, :hid], pre[:, hid:]
            scaled = gate_pre / (1.0 + jnp.exp(-gate_pre)) * up_pre * gcol[:, e : e + 1]
            hidden[:, e * hid : (e + 1) * hid] = scaled.astype(BF)

        def down(i, carry):
            columns = pl.ds(pl.multiple_of(i * tile, tile), tile)
            piece = jnp.dot(hidden[...], w_out[:, columns], preferred_element_type=F32).astype(
                BF
            )
            own[o, :, columns] = piece[: 2 * hr]
            oth[o, :, columns] = piece[2 * hr :]
            return carry

        lax.fori_loop(0, width // tile, down, 0)
        summed[o] = push(oth.at[o], got.at[o], sum_s.at[o], sum_r.at[o], partner)

    hops = {}
    settled = set()

    def settle(o):
        if o not in settled:
            summed[o].wait_recv()
            settled.add(o)

    def half_rows(hf, i):
        return pl.ds(pl.multiple_of(hf * hr + i * 16, 16), 16)

    def hop_send(dr, d, hf):
        o = (n_z - d) % n_z if dr == 1 else d
        settle(o)
        start = d == reach(dr, hf)
        if start:
            src = own.at[o, pl.ds(hf * hr, hr)]
        else:
            hops[(dr, d + 1, hf)].wait_recv()
            src = hop.at[dr, d, hf]

        def add(i, carry):
            local = pl.ds(pl.multiple_of(i * 16, 16), 16)
            total = own[o, half_rows(hf, i)].astype(F32) + got[o, half_rows(hf, i)].astype(F32)
            if not start:
                total = total + hop[dr, d, hf, local].astype(F32)
            src[local] = total.astype(BF)
            return carry

        lax.fori_loop(0, hr // 16, add, 0)
        sem = (dr, d, hf)
        hops[sem] = push(src, hop.at[dr, d - 1, hf], hop_s.at[sem], hop_r.at[sem], ring_dev[dr])

    compute(0)
    order = []
    for d in range(1, far):
        order += [(d, 0), (d, 1)]
    for d, sub in order:
        for dr in range(2):
            hf = sub
            ring_wait(dr, d, hf)
            if d < reach(dr, hf):
                ring_send(dr, d, hf)
            pair_send(at(dr, d), hf)
        if sub == 1:
            compute(at(0, d))
            compute(at(1, d))
    for dr in range(2):
        hop_send(dr, far - 1, 1 - dr)
    for dr in range(2):
        ring_wait(dr, far, dr)
        pair_send(at(dr, far), dr)
    compute(far)
    for dr in range(2):
        hop_send(dr, far, dr)
    for d in range(far - 2, 0, -1):
        for dr in range(2):
            hop_send(dr, d, 1 - dr)
        for dr in range(2):
            hop_send(dr, d + 1, dr)
    for dr in range(2):
        hop_send(dr, 1, dr)

    settle(0)
    returned = [None] * n_sp
    for hf in range(2):
        for dr in range(2):
            hops[(dr, 1, hf)].wait_recv()

        def finish(i, carry):
            local = pl.ds(pl.multiple_of(i * 16, 16), 16)
            total = own[0, half_rows(hf, i)].astype(F32) + got[0, half_rows(hf, i)].astype(F32)
            total = total + (hop[0, 0, hf, local].astype(F32) + hop[1, 0, hf, local].astype(F32))
            own[0, half_rows(hf, i)] = total.astype(BF)
            return carry

        lax.fori_loop(0, hr // 16, finish, 0)
        ret[pl.ds(hf * half * SLOT, half * SLOT)] = jnp.dot(
            pick_t[...], own[0, pl.ds(hf * hr, hr)], preferred_element_type=F32
        ).astype(BF)
        for j in range(hf * half, (hf + 1) * half):
            block = pl.ds(j * SLOT, SLOT)
            if j == 0:
                back[block] = ret[block]
            else:
                returned[j] = push(
                    ret.at[block], back.at[block], ret_s.at[j], ret_r.at[j], (lax.rem(sp + n_sp - j, n_sp), z, c)
                )
    for j in range(1, n_sp):
        returned[j].wait_recv()
    eye_tok = one_hot(iota((tok, tok), 0) == iota((tok, tok), 1))
    placing_t = lax.dot_general(eye_tok, placing[...], (((1,), (1,)), ((), ())), preferred_element_type=F32)
    expert_out = jnp.dot(placing_t.astype(BF), back[...], preferred_element_type=F32)
    out[...] = (mixed[...].astype(F32) + expert_out).astype(BF)
    for t in range(1, n_tp):
        a2a_copy(t, lax.rem(me + t, n_tp)).wait_send()
    for copy in sends:
        copy.wait_send()


def per_device(
    queries,
    key_heads,
    value_heads,
    sink_logit,
    out_weight,
    residual,
    mixer_gain,
    expert_gain,
    route_group,
    route_member,
    route_weight,
    gate_weight,
    up_weight,
    down_weight,
    n_x=4,
    cap=GROUP_CAP,
    kv_share=HEADS // KV_HEADS,
):
    n_sp, n_z = lax.axis_size("sp"), lax.axis_size("tp_0")
    n_y = n_sp // n_x
    n_tp = 2 * n_z
    tok, width = residual.shape
    seq = queries.shape[0]
    experts, hid = down_weight.shape[0], down_weight.shape[1]
    half = n_sp // 2
    hr = half * cap
    far = n_z // 2
    info = jnp.concatenate(
        [
            route_group.astype(F32)[None, :],
            route_member.astype(F32).T,
            route_weight.astype(F32).T,
            jnp.zeros((3, tok), F32),
        ],
        axis=0,
    )
    r = np.arange(hr)
    padded = r // cap * SLOT + r % cap
    i = np.arange(half * SLOT)
    e = np.arange(16)
    pick = jnp.asarray(i[None, :] == padded[:, None], BF)
    pick_t = jnp.asarray(i[:, None] == padded[None, :], BF)
    gate_pick = jnp.asarray((i[None, :] % SLOT == e[:, None] + cap) & (e[:, None] < experts), BF)
    vmem = pl.BlockSpec(memory_space=pltpu.VMEM)
    anywhere = pl.BlockSpec(memory_space=pl.ANY)
    dma = pltpu.SemaphoreType.DMA
    bf_bufs = [
        (seq, HEAD_DIM),
        (seq + 2 * WINDOW, HEAD_DIM),
        (seq + 2 * WINDOW, HEAD_DIM),
        (n_tp, BLOCK, HEAD_DIM),
        (tok, n_tp * HEAD_DIM),
        (n_y, n_x // 2, n_z, 2, 128, 256),
        None,
        (tok, width),
        (tok, width),
        (n_sp * SLOT, tok),
        None,
        (n_sp * SLOT, width),
        (n_sp * SLOT, width),
        (n_z, 4 * hr, width),
        (n_z, 2, 2, 16, 128),
        None,
        (4 * hr, experts * hid),
        (experts, width, 2 * hid),
        (experts * hid, width),
        (n_z, 2 * hr, width),
        (n_z, 2 * hr, width),
        (n_z, 2 * hr, width),
        (2, far, 2, hr, width),
        (n_sp * SLOT, width),
        (n_sp * SLOT, width),
    ]
    f32_bufs = iter([(tok, width), (n_sp * SLOT, 128), (4 * hr, 16)])
    buffers = [pltpu.VMEM(s, BF) if s is not None else pltpu.VMEM(next(f32_bufs), F32) for s in bf_bufs]
    sems = [(4,)]
    sems += [(2, 2)] * 2 + [(n_tp,)] * 2 + [(n_z,)] * 2 + [(2, 2, 2, 2)] * 4 + [(2, 2, 5)] * 2
    sems += [(experts, 3)] + [(n_sp,)] * 2 + [(2, far, 2)] * 4 + [(n_z, 2)] * 4 + [(n_z,)] * 2
    sems += [(2, far + 1, 2)] * 2 + [(n_sp,)] * 2
    return pl.pallas_call(
        functools.partial(layer_kernel, n_sp, n_x, n_z, kv_share, cap),
        out_shape=jax.ShapeDtypeStruct((tok, width), BF),
        in_specs=[anywhere] * 3 + [vmem, anywhere] + [vmem] * 7 + [anywhere] * 3,
        out_specs=vmem,
        scratch_shapes=buffers + [dma(s) for s in sems],
        compiler_params=pltpu.CompilerParams(
            collective_id=0, has_side_effects=True, vmem_limit_bytes=VMEM_LIMIT
        ),
    )(
        queries,
        key_heads,
        value_heads,
        sink_logit.reshape(1, 1),
        out_weight,
        residual,
        mixer_gain.reshape(1, -1),
        expert_gain.reshape(1, -1),
        info,
        pick,
        pick_t,
        gate_pick,
        gate_weight,
        up_weight,
        down_weight,
    )


def solution(mesh):
    torus = Mesh(mesh.devices.reshape(mesh.shape["sp"], 8, 2), ("sp", "tp_0", "tp_1"))
    placed = (
        P("sp", TP),
        P("sp", None),
        P("sp", None),
        P(TP),
        P(TP, None),
        P(SP_TP, None),
        P(),
        P(),
        P(SP_TP),
        P(SP_TP, None),
        P(SP_TP, None),
        P("sp", None, TP),
        P("sp", None, TP),
        P("sp", TP, None),
    )
    return jax.shard_map(
        per_device, mesh=torus, in_specs=placed, out_specs=P(SP_TP, None), check_vma=False
    )
```

```python
import functools

import jax
import jax.numpy as jnp
import numpy as np
from jax import lax
from jax.experimental import pallas as pl
from jax.experimental.pallas import tpu as pltpu
from jax.sharding import Mesh
from jax.sharding import PartitionSpec as P

HEADS = 16
KV_HEADS = 4
HEAD_DIM = 128
WINDOW = 128
BLOCK = 128
GROUP_EXPERTS = 3
GROUP_CAP = 10
SLOT = 16
CHUNKS = 4
TP = ("tp_0", "tp_1")
SP_TP = ("sp", "tp_0", "tp_1")
MESH_ID = pl.DeviceIdType.MESH
VMEM_LIMIT = 62 * 1024 * 1024

EPS = 1e-06
NEG_BIG = -1e30
BF = jnp.bfloat16
F32 = jnp.float32


def one_hot(condition):
    return jnp.where(condition, 1.0, 0.0).astype(BF)


def iota(shape, dim):
    return lax.broadcasted_iota(jnp.int32, shape, dim)


def layer_kernel(
    n_sp,
    n_x,
    n_z,
    kv_share,
    cap,
    queries,
    key_heads,
    value_heads,
    sink,
    out_weight,
    residual,
    mixer_gain,
    expert_gain,
    route_group,
    route_member,
    route_weight,
    pick,
    pick_t,
    gate_pick,
    wg,
    wu,
    wd,
    out,
    q_buf,
    k_buf,
    v_buf,
    att,
    by_token,
    w_proj,
    proj,
    normed,
    mixed,
    placing,
    gate_rows,
    send,
    arr,
    rows,
    gates,
    gcol,
    hidden,
    w_in,
    w_out,
    own,
    oth,
    got,
    hop,
    ret,
    back,
    load_sem,
    halo_s,
    halo_r,
    a2a_s,
    a2a_r,
    col_s,
    col_r,
    near_s,
    near_r,
    wide_s,
    wide_r,
    wpair_s,
    wpair_r,
    w_sem,
    disp_s,
    disp_r,
    ring_s,
    ring_r,
    rgate_s,
    rgate_r,
    pair_s,
    pair_r,
    pgate_s,
    pgate_r,
    sum_s,
    sum_r,
    hop_s,
    hop_r,
    ret_s,
    ret_r,
):
    sp, z, c = lax.axis_index("sp"), lax.axis_index("tp_0"), lax.axis_index("tp_1")
    me = z * 2 + c
    n_tp = 2 * n_z
    y, x = lax.div(sp, n_x), lax.rem(sp, n_x)
    n_y = n_sp // n_x
    tok, width = residual.shape
    experts, hid = wd.shape[0], wd.shape[1]
    half = n_sp // 2
    hr = half * cap
    far = n_z // 2
    tile = 256
    span = width // CHUNKS
    sends = []

    def remote(src, dst, s_sem, r_sem, dev):
        return pltpu.make_async_remote_copy(
            src_ref=src, dst_ref=dst, send_sem=s_sem, recv_sem=r_sem, device_id=dev, device_id_type=MESH_ID
        )

    def push(src, dst, s_sem, r_sem, dev):
        copy = remote(src, dst, s_sem, r_sem, dev)
        copy.start()
        sends.append(copy)
        return copy

    partner = (sp, z, 1 - c)
    ring_dev = ((sp, lax.rem(z + 1, n_z), c), (sp, lax.rem(z + n_z - 1, n_z), c))

    seq = q_buf.shape[0]
    head_at = pl.ds(pl.multiple_of(lax.div(me, kv_share) * HEAD_DIM, HEAD_DIM), HEAD_DIM)
    inner = pl.ds(WINDOW, seq)
    col_own = pl.ds(pl.multiple_of(sp * 128, 128), 128)
    lanes_own = pl.ds(pl.multiple_of(lax.rem(x, 2) * 128, 128), 128)
    w_own = w_proj.at[y, lax.div(x, 2), z, c, :, lanes_own]
    first = [
        pltpu.make_async_copy(key_heads.at[:, head_at], k_buf.at[inner], load_sem.at[0]),
        pltpu.make_async_copy(value_heads.at[:, head_at], v_buf.at[inner], load_sem.at[1]),
        pltpu.make_async_copy(out_weight.at[:, col_own], w_own, load_sem.at[2]),
        pltpu.make_async_copy(queries, q_buf, load_sem.at[3]),
    ]
    for load in first:
        load.start()
    loads = []
    for e in range(experts):
        loads.append(pltpu.make_async_copy(wg.at[e], w_in.at[e, :, pl.ds(0, hid)], w_sem.at[e, 0]))
        loads.append(pltpu.make_async_copy(wu.at[e], w_in.at[e, :, pl.ds(hid, hid)], w_sem.at[e, 1]))
        loads.append(pltpu.make_async_copy(wd.at[e], w_out.at[pl.ds(e * hid, hid), :], w_sem.at[e, 2]))

    barrier = pltpu.get_barrier_semaphore()
    for j in range(1, n_sp):
        pl.semaphore_signal(barrier, inc=1, device_id=(lax.rem(sp + j, n_sp), z, c), device_id_type=MESH_ID)
    for j in range(1, n_tp):
        n = lax.rem(me + j, n_tp)
        pl.semaphore_signal(
            barrier, inc=1, device_id=(sp, lax.div(n, 2), lax.rem(n, 2)), device_id_type=MESH_ID
        )
    for load in first:
        load.wait()
    pl.semaphore_wait(barrier, n_sp - 1 + n_tp - 1)

    after, before = lax.rem(sp + 1, n_sp), lax.rem(sp + n_sp - 1, n_sp)
    low, high = pl.ds(0, WINDOW), pl.ds(WINDOW + seq, WINDOW)
    halo = []
    for i, buf in enumerate((k_buf, v_buf)):
        halo.append(push(buf.at[pl.ds(seq, WINDOW)], buf.at[low], halo_s.at[0, i], halo_r.at[0, i], (after, z, c)))
        halo.append(push(buf.at[pl.ds(WINDOW, WINDOW)], buf.at[high], halo_s.at[1, i], halo_r.at[1, i], (before, z, c)))

    def col_region(d):
        return w_proj.at[y, lax.div(x, 2), lax.rem(z + n_z - d, n_z), c, :, lanes_own]

    column = []
    for k in range(1, n_z):
        d = (k + 1) // 2 if k % 2 else n_z - k // 2
        push(w_own, w_own, col_s.at[d], col_r.at[d], (sp, lax.rem(z + d, n_z), c))
        column.append(d)
    for load in loads:
        load.start()

    sink_val = sink[0, 0]
    q_pos = iota((BLOCK, BLOCK + 2 * WINDOW), 0)
    k_pos = iota((BLOCK, BLOCK + 2 * WINDOW), 1)

    def attend(n):
        @pl.when(n == 0)
        def _():
            for i in range(2):
                halo[2 * i].wait_recv()

        @pl.when(n == n_tp - 1)
        def _():
            for i in range(2):
                halo[2 * i + 1].wait_recv()

        start = pl.multiple_of(n * BLOCK, BLOCK)
        keys = pl.ds(start, BLOCK + 2 * WINDOW)
        scores = lax.dot_general(
            q_buf[pl.ds(start, BLOCK), :], k_buf[keys, :], (((1,), (1,)), ((), ())), preferred_element_type=F32
        ) * HEAD_DIM ** (-0.5)
        lo = jnp.where((sp == 0) & (n == 0), WINDOW, 0)
        hi = jnp.where((sp == n_sp - 1) & (n == n_tp - 1), BLOCK + WINDOW, BLOCK + 2 * WINDOW)
        inside = (k_pos >= q_pos) & (k_pos <= q_pos + 2 * WINDOW) & (k_pos >= lo) & (k_pos < hi)
        scores = jnp.where(inside, scores, NEG_BIG)
        top = jnp.maximum(jnp.max(scores, axis=1, keepdims=True), sink_val)
        terms = jnp.exp(scores - top)
        mass = jnp.sum(terms, axis=1, keepdims=True) + jnp.exp(sink_val - top)
        value = jnp.dot(terms.astype(BF), v_buf[keys, :], preferred_element_type=F32)
        return (value / mass).astype(BF)

    my_cols = pl.ds(pl.multiple_of(me * HEAD_DIM, HEAD_DIM), HEAD_DIM)

    def a2a_copy(t, n):
        return remote(
            att.at[n], by_token.at[:, my_cols], a2a_s.at[t], a2a_r.at[t], (sp, lax.div(n, 2), lax.rem(n, 2))
        )

    def attend_pair(t, carry):
        ahead, behind = lax.rem(me + t, n_tp), lax.rem(me + n_tp - t, n_tp)
        first_val, second_val = attend(ahead), attend(behind)
        att[ahead] = first_val
        att[behind] = second_val
        a2a_copy(t, ahead).start()
        a2a_copy(n_tp - t, behind).start()
        return carry

    axis_len = (n_x, n_y)
    place = (x, y)
    zq = n_z // 4

    def plane_dev(axis, step):
        at_axis = lax.rem(place[axis] + step + axis_len[axis], axis_len[axis])
        return (y * n_x + at_axis, z, c) if axis == 0 else (at_axis * n_x + x, z, c)

    def plane_region(order, wide, d, dr, hf):
        axis = order if not wide else 1 - order
        at_axis = lax.rem(place[axis] + (axis_len[axis] - d if dr == 0 else d), axis_len[axis])
        zr = pl.ds(order * 2 * zq + hf * zq, zq)
        if wide:
            if axis == 1:
                return w_proj.at[at_axis, :, zr, c]
            lanes = pl.ds(pl.multiple_of(lax.rem(at_axis, 2) * 128, 128), 128)
            return w_proj.at[:, lax.div(at_axis, 2), zr, c, :, lanes]
        if axis == 0:
            lanes = pl.ds(pl.multiple_of(lax.rem(at_axis, 2) * 128, 128), 128)
            return w_proj.at[y, lax.div(at_axis, 2), zr, c, :, lanes]
        return w_proj.at[at_axis, lax.div(x, 2), zr, c, :, lanes_own]

    def plane_reach(order, wide, dr, hf):
        axis = order if not wide else 1 - order
        limit = axis_len[axis] // 2
        return limit if dr == hf else limit - 1

    def plane_copy(order, wide, d, dr, hf):
        axis = order if not wide else 1 - order
        region = plane_region(order, wide, d, dr, hf)
        s_sem, r_sem = (wide_s, wide_r) if wide else (near_s, near_r)
        sem = (order, dr, d, hf)
        return remote(region, region, s_sem.at[sem], r_sem.at[sem], plane_dev(axis, 1 if dr == 0 else -1))

    def plane_send(order, wide, d, dr, hf):
        if d < plane_reach(order, wide, dr, hf):
            copy = plane_copy(order, wide, d, dr, hf)
            copy.start()
            sends.append(copy)

    def plane_wait(order, wide, d, dr, hf):
        axis = order if not wide else 1 - order
        region = plane_region(order, wide, d, dr, hf)
        s_sem, r_sem = (wide_s, wide_r) if wide else (near_s, near_r)
        sem = (order, dr, d - 1, hf)
        remote(region, region, s_sem.at[sem], r_sem.at[sem], plane_dev(axis, 1 if dr == 0 else -1)).wait_recv()

    def plane_steps(order, wide):
        limit = axis_len[order if not wide else 1 - order] // 2
        steps = []
        for d in range(1, limit + 1):
            for sub in range(2):
                for dr in range(2):
                    hf = dr if sub == 0 else 1 - dr
                    if d <= plane_reach(order, wide, dr, hf):
                        steps.append((d, dr, hf))
        return steps

    wpairs = []

    def wpair_send(region, index):
        wpairs.append(push(region, region, wpair_s.at[index], wpair_r.at[index], partner))

    def wpair_wait(order, d, dr, hf, index):
        axis = 1 - order
        at_axis = lax.rem(place[axis] + (axis_len[axis] - d if dr == 0 else d), axis_len[axis])
        zr = pl.ds(order * 2 * zq + hf * zq, zq)
        if axis == 1:
            region = w_proj.at[at_axis, :, zr, 1 - c]
        else:
            lanes = pl.ds(pl.multiple_of(lax.rem(at_axis, 2) * 128, 128), 128)
            region = w_proj.at[:, lax.div(at_axis, 2), zr, 1 - c, :, lanes]
        remote(region, region, wpair_s.at[index], wpair_r.at[index], partner).wait_recv()

    split = max(1, (n_tp // 2) // 2)
    lax.fori_loop(1, 1 + split, attend_pair, 0)
    for d in column:
        remote(w_own, col_region(d), col_s.at[d], col_r.at[d], ring_dev[0]).wait_recv()
    for hf_step in range(2):
        for order in range(2):
            for dr in range(2):
                plane_send(order, False, 0, dr, dr if hf_step == 0 else 1 - dr)
    lax.fori_loop(1 + split, n_tp // 2, attend_pair, 0)
    opposite = lax.rem(me + n_tp // 2, n_tp)
    first_val, own_val = attend(opposite), attend(me)
    att[opposite] = first_val
    by_token[:, my_cols] = own_val
    a2a_copy(n_tp // 2, opposite).start()

    for step in plane_steps(0, False):
        for order in range(2):
            d, dr, hf = step
            plane_wait(order, False, d, dr, hf)
            plane_send(order, False, d, dr, hf)
    for hf_step in range(2):
        for order in range(2):
            for dr in range(2):
                plane_send(order, True, 0, dr, dr if hf_step == 0 else 1 - dr)
    for order in range(2):
        for hf in range(2):
            wpair_send(plane_region(order, True, 0, 0, hf), (order, hf, 0))

    ahead = route_group[...] - sp
    ahead = jnp.where(ahead < 0, ahead + n_sp, ahead)
    chosen = iota((n_sp, tok), 0) == ahead
    earlier = one_hot(iota((tok, tok), 0) < iota((tok, tok), 1))
    ranks = jnp.dot(one_hot(chosen), earlier, preferred_element_type=F32)
    rank = jnp.sum(jnp.where(chosen, ranks, 0.0), axis=0, keepdims=True).astype(jnp.int32)
    slot_row = iota((n_sp * SLOT, tok), 0)
    placing[...] = one_hot(slot_row == ahead * SLOT + rank)
    in_half = jnp.where(ahead >= half, ahead - half, ahead)
    lane_hot = one_hot(iota((128, tok), 0) == in_half * cap + rank)
    gate_at = jnp.zeros((n_sp * SLOT, tok), F32)
    for k in range(2):
        member = route_member[k : k + 1, :]
        weight = route_weight[k : k + 1, :].astype(F32)
        gate_at = gate_at + jnp.where(slot_row == ahead * SLOT + cap + member, weight, 0.0)
    gate_rows[...] = lax.dot_general(
        gate_at.astype(BF), lane_hot, (((1,), (1,)), ((), ())), preferred_element_type=F32
    )

    for step in plane_steps(0, True):
        for order in range(2):
            d, dr, hf = step
            plane_wait(order, True, d, dr, hf)
            plane_send(order, True, d, dr, hf)
            index = (order, hf, 1 + (d - 1) * 2 + dr)
            wpair_send(plane_region(order, True, d, dr, hf), index)
    for t in range(1, n_tp):
        source = pl.ds(pl.multiple_of(lax.rem(me + n_tp - t, n_tp) * HEAD_DIM, HEAD_DIM), HEAD_DIM)
        remote(att.at[0], by_token.at[:, source], a2a_s.at[t], a2a_r.at[t], partner).wait_recv()
    for order in range(2):
        for hf in range(2):
            wpair_wait(order, 0, 0, hf, (order, hf, 0))
    for d, dr, hf in plane_steps(0, True):
        for order in range(2):
            wpair_wait(order, d, dr, hf, (order, hf, 1 + (d - 1) * 2 + dr))

    w_tiles = width // tile

    def project(i, carry):
        block = w_proj[lax.div(i, w_tiles // n_y), lax.rem(i, w_tiles // n_y)].reshape(n_tp * HEAD_DIM, tile)
        columns = pl.ds(pl.multiple_of(i * tile, tile), tile)
        proj[:, columns] = jnp.dot(by_token[...], block, preferred_element_type=F32)
        return carry

    lax.fori_loop(0, w_tiles, project, 0)

    def norms(i, carry):
        at_rows = pl.ds(pl.multiple_of(i * 16, 16), 16)
        value = proj[at_rows, :]
        scale = lax.rsqrt(jnp.mean(value * value, axis=1, keepdims=True) + EPS)
        mixed_bf = (residual[at_rows, :].astype(F32) + mixer_gain[...] * (value * scale)).astype(BF)
        mixed[at_rows, :] = mixed_bf
        mixed_f = mixed_bf.astype(F32)
        scale = lax.rsqrt(jnp.mean(mixed_f * mixed_f, axis=1, keepdims=True) + EPS)
        normed[at_rows, :] = (mixed_f * scale * expert_gain[...]).astype(BF)
        return carry

    lax.fori_loop(0, tok // 16, norms, 0)

    head = jnp.dot(placing[...], normed[:, 0:128], preferred_element_type=F32)
    send[:, 0:128] = (head + gate_rows[...]).astype(BF)
    send[:, 128:] = jnp.dot(placing[...], normed[:, 128:], preferred_element_type=F32).astype(BF)
    def cut(ch):
        return pl.ds(ch * span, span)

    disp = {}
    for hf in range(2):
        for ch in range(CHUNKS):
            for j in range(hf * half, (hf + 1) * half):
                at_slot = (pl.ds(j * SLOT, SLOT), cut(ch))
                if j > 0:
                    disp[(ch, j)] = push(
                        send.at[at_slot],
                        arr.at[at_slot],
                        disp_s.at[ch, j],
                        disp_r.at[ch, j],
                        (lax.rem(sp + j, n_sp), z, c),
                    )
    arr[0:SLOT] = send[0:SLOT]

    def reach(dr, hf):
        return far if dr == hf else far - 1

    def at(dr, d):
        return (n_z - d) % n_z if dr == 0 else d

    arrivals = [(1, 0), (1, 1)] + [(d, 0) for d in range(2, far + 1)] + [(d, 1) for d in range(2, far)]
    together = [[(0, 0), (0, 1)]]
    for d, kind in arrivals:
        together.append([(at(dr, d), kind if d == 1 or dr == 0 else 1 - kind) for dr in range(2)])
    place_at = {unit: (i, sub) for i, units in enumerate(together) for sub, unit in enumerate(units)}

    def spot(o, rc, hf):
        i, sub = place_at[(o, hf)]
        return i, pl.ds((sub * 2 + rc) * hr, hr)

    def sum_spot(o, hf):
        i, sub = place_at[(o, hf)]
        return i, pl.ds(sub * hr, hr)

    ring = {}
    ring_g = {}
    pair = {}

    def ring_send(dr, d, hf, ch):
        src, dst = at(dr, d), at(dr, d + 1)
        sem = (dr, d, hf, ch)
        ring[sem] = push(
            rows.at[(*spot(src, 0, hf), cut(ch))],
            rows.at[(*spot(dst, 0, hf), cut(ch))],
            ring_s.at[sem],
            ring_r.at[sem],
            ring_dev[dr],
        )
        if ch == 0:
            sem = (dr, d, hf)
            ring_g[sem] = push(
                gates.at[src, 0, hf], gates.at[dst, 0, hf], rgate_s.at[sem], rgate_r.at[sem], ring_dev[dr]
            )

    def ring_wait(dr, d, hf, ch):
        ring[(dr, d - 1, hf, ch)].wait_recv()
        if ch == 0:
            ring_g[(dr, d - 1, hf)].wait_recv()

    def pair_send(o, hf):
        pair[(o, hf)] = (
            push(rows.at[spot(o, 0, hf)], rows.at[spot(o, 1, hf)], pair_s.at[o, hf], pair_r.at[o, hf], partner),
            push(gates.at[o, 0, hf], gates.at[o, 1, hf], pgate_s.at[o, hf], pgate_r.at[o, hf], partner),
        )

    for hf in range(2):
        block = pl.ds(hf * half * SLOT, half * SLOT)
        for ch in range(CHUNKS):
            for j in range(hf * half, (hf + 1) * half):
                if j > 0:
                    disp[(ch, j)].wait_recv()
            if ch == 0:
                gates[0, 0, hf] = jnp.dot(
                    gate_pick[...], arr[block, 0:128], preferred_element_type=F32
                ).astype(BF)
            rows[(*spot(0, 0, hf), cut(ch))] = jnp.dot(
                pick[...], arr[block, cut(ch)], preferred_element_type=F32
            ).astype(BF)
            ring_send(0, 0, hf, ch)
            ring_send(1, 0, hf, ch)
        pair_send(0, hf)

    for load in loads:
        load.wait()

    eye = one_hot(iota((hr, 128), 0) == iota((hr, 128), 1))
    summed = {}

    def compute(step):
        for sub, (o, hf) in enumerate(together[step]):
            for copy in pair[(o, hf)]:
                copy.wait_recv()
            for rc in range(2):
                gcol[pl.ds((sub * 2 + rc) * hr, hr)] = lax.dot_general(
                    eye, gates[o, rc, hf], (((1,), (1,)), ((), ())), preferred_element_type=F32
                )
        for e in range(experts):
            pre = jnp.dot(rows[step], w_in[e], preferred_element_type=F32)
            gate_pre, up_pre = pre[:, :hid], pre[:, hid:]
            scaled = gate_pre / (1.0 + jnp.exp(-gate_pre)) * up_pre * gcol[:, e : e + 1]
            hidden[:, e * hid : (e + 1) * hid] = scaled.astype(BF)

        def down(i, carry):
            columns = pl.ds(pl.multiple_of(i * tile, tile), tile)
            piece = jnp.dot(hidden[...], w_out[:, columns], preferred_element_type=F32).astype(BF)
            for sub in range(2):
                own[step, pl.ds(sub * hr, hr), columns] = piece[sub * 2 * hr : (sub * 2 + 1) * hr]
                oth[step, pl.ds(sub * hr, hr), columns] = piece[(sub * 2 + 1) * hr : (sub * 2 + 2) * hr]
            return carry

        lax.fori_loop(0, width // tile, down, 0)
        summed[step] = push(oth.at[step], got.at[step], sum_s.at[step], sum_r.at[step], partner)

    hops = {}
    settled = set()

    def settle(o, hf):
        step = place_at[(o, hf)][0]
        if step not in settled:
            summed[step].wait_recv()
            settled.add(step)

    def own_rows(o, hf, i):
        step, sub = place_at[(o, hf)]
        return step, pl.ds(pl.multiple_of(sub * hr + i * 16, 16), 16)

    def hop_send(dr, d, hf, ch):
        o = (n_z - d) % n_z if dr == 1 else d
        settle(o, hf)
        start = d == reach(1 - dr, hf)
        if start:
            src = own.at[(*sum_spot(o, hf), cut(ch))]
        else:
            hops[(dr, d + 1, hf, ch)].wait_recv()
            src = hop.at[dr, d, hf, :, cut(ch)]

        def add(i, carry):
            local = pl.ds(pl.multiple_of(i * 16, 16), 16)
            at_rows = (*own_rows(o, hf, i), cut(ch))
            total = own[at_rows].astype(F32) + got[at_rows].astype(F32)
            if not start:
                total = total + hop[dr, d, hf, local, cut(ch)].astype(F32)
            src[local] = total.astype(BF)
            return carry

        lax.fori_loop(0, hr // 16, add, 0)
        sem = (dr, d, hf, ch)
        hops[sem] = push(src, hop.at[dr, d - 1, hf, :, cut(ch)], hop_s.at[sem], hop_r.at[sem], ring_dev[dr])

    returned = {}

    def finish(ch):
        for hf in range(2):
            settle(0, hf)
            for dr in range(2):
                hops[(dr, 1, hf, ch)].wait_recv()

            def last_add(i, carry):
                local = pl.ds(pl.multiple_of(i * 16, 16), 16)
                at_rows = (*own_rows(0, hf, i), cut(ch))
                total = own[at_rows].astype(F32) + got[at_rows].astype(F32)
                total = total + (
                    hop[0, 0, hf, local, cut(ch)].astype(F32) + hop[1, 0, hf, local, cut(ch)].astype(F32)
                )
                own[at_rows] = total.astype(BF)
                return carry

            lax.fori_loop(0, hr // 16, last_add, 0)
            ret[pl.ds(hf * half * SLOT, half * SLOT), cut(ch)] = jnp.dot(
                pick_t[...], own[(*sum_spot(0, hf), cut(ch))], preferred_element_type=F32
            ).astype(BF)
            for j in range(hf * half, (hf + 1) * half):
                at_slot = (pl.ds(j * SLOT, SLOT), cut(ch))
                if j == 0:
                    back[0:SLOT, cut(ch)] = ret[0:SLOT, cut(ch)]
                else:
                    returned[(ch, j)] = push(
                        ret.at[at_slot],
                        back.at[at_slot],
                        ret_s.at[ch, j],
                        ret_r.at[ch, j],
                        (lax.rem(sp + n_sp - j, n_sp), z, c),
                    )

    compute(0)

    def long_hop(d, ch):
        for dr in range(2):
            hop_send(dr, d, 1 - dr, ch)

    done = {0}

    def need(step):
        if step not in done:
            compute(step)
            done.add(step)

    far_step = place_at[(far, 0)][0]
    for k, (d, kind) in enumerate(arrivals):
        step = k + 1
        for ch in range(CHUNKS):
            if step == far_step + 1 and ch == CHUNKS // 2:
                need(far_step)
            for dr in range(2):
                hf = together[step][dr][1]
                ring_wait(dr, d, hf, ch)
                if d < reach(dr, hf) and not (d == 1 and dr != hf):
                    ring_send(dr, d, hf, ch)
        if (d, kind) == (far - 1, 0):
            for ch in range(CHUNKS):
                for dr in range(2):
                    if 1 < reach(dr, 1 - dr):
                        ring_send(dr, 1, 1 - dr, ch)
        for o, hf in together[step]:
            pair_send(o, hf)
        if k > 0 and step != far_step + 1 and step != len(arrivals):
            need(step - 1)
        if step == len(arrivals) - 1 and far > 2:
            for ch in range(CHUNKS):
                long_hop(far, ch)
            need(step)
    if far == 2:
        need(1)
        need(2)
        need(3)
        for ch in range(CHUNKS):
            long_hop(far, ch)
    for ch in range(CHUNKS // 2):
        long_hop(far - 1, ch)
    need(len(arrivals))
    for ch in range(CHUNKS // 2, CHUNKS):
        long_hop(far - 1, ch)
    events = []
    for ch in range(CHUNKS):
        at_key = 1.2 * ch
        for d in range(far - 1, 0, -1):
            events.append((at_key, ch, d, 1))
            at_key += 1
            if d > 1:
                events.append((at_key, ch, d - 1, 0))
                at_key += 1
        events.append((at_key + 0.3, ch, 0, 0))
    for _, ch, d, kind in sorted(events):
        if d == 0:
            finish(ch)
        else:
            for dr in range(2):
                hop_send(dr, d, 1 - dr if kind == 0 else dr, ch)
    eye_tok = one_hot(iota((tok, tok), 0) == iota((tok, tok), 1))
    placing_t = lax.dot_general(
        eye_tok, placing[...], (((1,), (1,)), ((), ())), preferred_element_type=F32
    ).astype(BF)
    for ch in range(CHUNKS):
        for j in range(1, n_sp):
            returned[(ch, j)].wait_recv()
        expert_out = jnp.dot(placing_t, back[:, cut(ch)], preferred_element_type=F32)
        out[:, cut(ch)] = (mixed[:, cut(ch)].astype(F32) + expert_out).astype(BF)
    for t in range(1, n_tp):
        a2a_copy(t, lax.rem(me + t, n_tp)).wait_send()
    for copy in sends:
        copy.wait_send()


def per_device(
    queries,
    key_heads,
    value_heads,
    sink_logit,
    out_weight,
    residual,
    mixer_gain,
    expert_gain,
    route_group,
    route_member,
    route_weight,
    gate_weight,
    up_weight,
    down_weight,
    n_x=4,
    cap=GROUP_CAP,
    kv_share=HEADS // KV_HEADS,
):
    n_sp, n_z = lax.axis_size("sp"), lax.axis_size("tp_0")
    n_y = n_sp // n_x
    n_tp = 2 * n_z
    tok, width = residual.shape
    seq = queries.shape[0]
    experts, hid = down_weight.shape[0], down_weight.shape[1]
    half = n_sp // 2
    hr = half * cap
    far = n_z // 2
    r = np.arange(hr)
    padded = r // cap * SLOT + r % cap
    i = np.arange(half * SLOT)
    e = np.arange(16)
    pick = jnp.asarray(i[None, :] == padded[:, None], BF)
    pick_t = jnp.asarray(i[:, None] == padded[None, :], BF)
    gate_pick = jnp.asarray((i[None, :] % SLOT == e[:, None] + cap) & (e[:, None] < experts), BF)
    vmem = pl.BlockSpec(memory_space=pltpu.VMEM)
    anywhere = pl.BlockSpec(memory_space=pl.ANY)
    dma = pltpu.SemaphoreType.DMA
    bf_bufs = [
        (seq, HEAD_DIM),
        (seq + 2 * WINDOW, HEAD_DIM),
        (seq + 2 * WINDOW, HEAD_DIM),
        (n_tp, BLOCK, HEAD_DIM),
        (tok, n_tp * HEAD_DIM),
        (n_y, n_x // 2, n_z, 2, 128, 256),
        None,
        (tok, width),
        (tok, width),
        (n_sp * SLOT, tok),
        None,
        (n_sp * SLOT, width),
        (n_sp * SLOT, width),
        (n_z, 4 * hr, width),
        (n_z, 2, 2, 16, 128),
        None,
        (4 * hr, experts * hid),
        (experts, width, 2 * hid),
        (experts * hid, width),
        (n_z, 2 * hr, width),
        (n_z, 2 * hr, width),
        (n_z, 2 * hr, width),
        (2, far, 2, hr, width),
        (n_sp * SLOT, width),
        (n_sp * SLOT, width),
    ]
    f32_bufs = iter([(tok, width), (n_sp * SLOT, 128), (4 * hr, 16)])
    buffers = [pltpu.VMEM(s, BF) if s is not None else pltpu.VMEM(next(f32_bufs), F32) for s in bf_bufs]
    sems = [(4,)]
    sems += [(2, 2)] * 2 + [(n_tp,)] * 2 + [(n_z,)] * 2 + [(2, 2, 2, 2)] * 4 + [(2, 2, 5)] * 2
    sems += [(experts, 3)] + [(CHUNKS, n_sp)] * 2 + [(2, far, 2, CHUNKS)] * 2 + [(2, far, 2)] * 2 + [(n_z, 2)] * 4 + [(n_z,)] * 2
    sems += [(2, far + 1, 2, CHUNKS)] * 2 + [(CHUNKS, n_sp)] * 2
    return pl.pallas_call(
        functools.partial(layer_kernel, n_sp, n_x, n_z, kv_share, cap),
        out_shape=jax.ShapeDtypeStruct((tok, width), BF),
        in_specs=[anywhere] * 3 + [vmem, anywhere] + [vmem] * 9 + [anywhere] * 3,
        out_specs=vmem,
        scratch_shapes=buffers + [dma(s) for s in sems],
        compiler_params=pltpu.CompilerParams(
            collective_id=0, has_side_effects=True, vmem_limit_bytes=VMEM_LIMIT
        ),
    )(
        queries,
        key_heads,
        value_heads,
        sink_logit.reshape(1, 1),
        out_weight,
        residual,
        mixer_gain.reshape(1, -1),
        expert_gain.reshape(1, -1),
        route_group.reshape(1, -1),
        route_member.T,
        route_weight.T,
        pick,
        pick_t,
        gate_pick,
        gate_weight,
        up_weight,
        down_weight,
    )


def solution(mesh):
    torus = Mesh(mesh.devices.reshape(mesh.shape["sp"], 8, 2), ("sp", "tp_0", "tp_1"))
    placed = (
        P("sp", TP),
        P("sp", None),
        P("sp", None),
        P(TP),
        P(TP, None),
        P(SP_TP, None),
        P(),
        P(),
        P(SP_TP),
        P(SP_TP, None),
        P(SP_TP, None),
        P("sp", None, TP),
        P("sp", None, TP),
        P("sp", TP, None),
    )
    return jax.shard_map(
        per_device, mesh=torus, in_specs=placed, out_specs=P(SP_TP, None), check_vma=False
    )
```

```python
import functools

import jax
import jax.numpy as jnp
import numpy as np
from jax import lax
from jax.experimental import pallas as pl
from jax.experimental.pallas import tpu as pltpu
from jax.sharding import Mesh
from jax.sharding import PartitionSpec as P

HEADS = 16
KV_HEADS = 4
HEAD_DIM = 128
WINDOW = 128
BLOCK = 128
GROUP_EXPERTS = 3
GROUP_CAP = 10
SLOT = 16
CHUNKS = 4
Z_ROWS = 32
TP = ("tp_0", "tp_1")
SP_TP = ("sp", "tp_0", "tp_1")
MESH_ID = pl.DeviceIdType.MESH
VMEM_LIMIT = 62 * 1024 * 1024

EPS = 1e-06
NEG_BIG = -1e30
BF = jnp.bfloat16
F32 = jnp.float32


def one_hot(condition):
    return jnp.where(condition, 1.0, 0.0).astype(BF)


def iota(shape, dim):
    return lax.broadcasted_iota(jnp.int32, shape, dim)


def layer_kernel(
    n_sp,
    n_x,
    n_z,
    kv_share,
    cap,
    queries,
    key_heads,
    value_heads,
    sink,
    out_weight,
    residual,
    mixer_gain,
    expert_gain,
    route_group,
    route_member,
    route_weight,
    pick,
    pick_t,
    gate_pick,
    wg,
    wu,
    wd,
    out,
    q_buf,
    k_buf,
    v_buf,
    att,
    by_token,
    w_proj,
    proj,
    normed,
    mixed,
    placing,
    gate_rows,
    send,
    arr,
    rows,
    gates,
    gcol,
    hidden,
    w_in,
    w_out,
    own,
    oth,
    got,
    hop,
    ret,
    back,
    load_sem,
    halo_s,
    halo_r,
    a2a_s,
    a2a_r,
    col_s,
    col_r,
    near_s,
    near_r,
    wide_s,
    wide_r,
    wpair_s,
    wpair_r,
    zrow_s,
    zrow_r,
    zpair_s,
    zpair_r,
    zload_sem,
    w_sem,
    disp_s,
    disp_r,
    ring_s,
    ring_r,
    rgate_s,
    rgate_r,
    pair_s,
    pair_r,
    pgate_s,
    pgate_r,
    sum_s,
    sum_r,
    hop_s,
    hop_r,
    ret_s,
    ret_r,
):
    sp, z, c = lax.axis_index("sp"), lax.axis_index("tp_0"), lax.axis_index("tp_1")
    me = z * 2 + c
    n_tp = 2 * n_z
    y, x = lax.div(sp, n_x), lax.rem(sp, n_x)
    n_y = n_sp // n_x
    tok, width = residual.shape
    experts, hid = wd.shape[0], wd.shape[1]
    half = n_sp // 2
    hr = half * cap
    far = n_z // 2
    tile = 256
    span = width // CHUNKS
    sends = []

    def remote(src, dst, s_sem, r_sem, dev):
        return pltpu.make_async_remote_copy(
            src_ref=src, dst_ref=dst, send_sem=s_sem, recv_sem=r_sem, device_id=dev, device_id_type=MESH_ID
        )

    def push(src, dst, s_sem, r_sem, dev):
        copy = remote(src, dst, s_sem, r_sem, dev)
        copy.start()
        sends.append(copy)
        return copy

    partner = (sp, z, 1 - c)
    ring_dev = ((sp, lax.rem(z + 1, n_z), c), (sp, lax.rem(z + n_z - 1, n_z), c))

    seq = q_buf.shape[0]
    head_at = pl.ds(pl.multiple_of(lax.div(me, kv_share) * HEAD_DIM, HEAD_DIM), HEAD_DIM)
    inner = pl.ds(WINDOW, seq)
    col_own = pl.ds(pl.multiple_of(sp * 128, 128), 128)
    lanes_own = pl.ds(pl.multiple_of(lax.rem(x, 2) * 128, 128), 128)
    plane_rows = pl.ds(Z_ROWS, HEAD_DIM - Z_ROWS)
    ring_rows = pl.ds(0, Z_ROWS)
    w_own = w_proj.at[y, lax.div(x, 2), z, c, plane_rows, lanes_own]
    first = [
        pltpu.make_async_copy(key_heads.at[:, head_at], k_buf.at[inner], load_sem.at[0]),
        pltpu.make_async_copy(value_heads.at[:, head_at], v_buf.at[inner], load_sem.at[1]),
        pltpu.make_async_copy(out_weight.at[plane_rows, col_own], w_own, load_sem.at[2]),
        pltpu.make_async_copy(queries, q_buf, load_sem.at[3]),
    ]
    for i in range(width // tile):
        per_y = width // tile // n_y
        first.append(
            pltpu.make_async_copy(
                out_weight.at[ring_rows, pl.ds(i * tile, tile)],
                w_proj.at[i // per_y, i % per_y, z, c, ring_rows, :],
                zload_sem.at[i],
            )
        )
    for load in first:
        load.start()
    loads = []
    for e in range(experts):
        loads.append(pltpu.make_async_copy(wg.at[e], w_in.at[e, :, pl.ds(0, hid)], w_sem.at[e, 0]))
        loads.append(pltpu.make_async_copy(wu.at[e], w_in.at[e, :, pl.ds(hid, hid)], w_sem.at[e, 1]))
        loads.append(pltpu.make_async_copy(wd.at[e], w_out.at[pl.ds(e * hid, hid), :], w_sem.at[e, 2]))

    barrier = pltpu.get_barrier_semaphore()
    for j in range(1, n_sp):
        pl.semaphore_signal(barrier, inc=1, device_id=(lax.rem(sp + j, n_sp), z, c), device_id_type=MESH_ID)
    for j in range(1, n_tp):
        n = lax.rem(me + j, n_tp)
        pl.semaphore_signal(
            barrier, inc=1, device_id=(sp, lax.div(n, 2), lax.rem(n, 2)), device_id_type=MESH_ID
        )
    for load in first:
        load.wait()
    pl.semaphore_wait(barrier, n_sp - 1 + n_tp - 1)

    after, before = lax.rem(sp + 1, n_sp), lax.rem(sp + n_sp - 1, n_sp)
    low, high = pl.ds(0, WINDOW), pl.ds(WINDOW + seq, WINDOW)
    halo = []
    for i, buf in enumerate((k_buf, v_buf)):
        halo.append(push(buf.at[pl.ds(seq, WINDOW)], buf.at[low], halo_s.at[0, i], halo_r.at[0, i], (after, z, c)))
        halo.append(push(buf.at[pl.ds(WINDOW, WINDOW)], buf.at[high], halo_s.at[1, i], halo_r.at[1, i], (before, z, c)))

    def col_region(d):
        return w_proj.at[y, lax.div(x, 2), lax.rem(z + n_z - d, n_z), c, plane_rows, lanes_own]

    column = []
    for k in range(1, n_z):
        d = (k + 1) // 2 if k % 2 else n_z - k // 2
        push(w_own, w_own, col_s.at[d], col_r.at[d], (sp, lax.rem(z + d, n_z), c))
        column.append(d)
    def zrow_reach(dr, hf):
        return far if dr == hf else far - 1

    def zrow_region(dr, d, hf):
        at_z = lax.rem(z + (n_z - d if dr == 0 else d), n_z)
        return w_proj.at[pl.ds(hf * (n_y // 2), n_y // 2), :, at_z, c, ring_rows, :]

    def zrow_step(d):
        for sub in range(2):
            for dr in range(2):
                hf = dr if sub == 0 else 1 - dr
                region = zrow_region(dr, d, hf)
                if 0 < d <= zrow_reach(dr, hf):
                    sem = (dr, d - 1, hf)
                    remote(region, region, zrow_s.at[sem], zrow_r.at[sem], ring_dev[dr]).wait_recv()
                if d < zrow_reach(dr, hf):
                    sem = (dr, d, hf)
                    push(region, region, zrow_s.at[sem], zrow_r.at[sem], ring_dev[dr])

    zrow_step(0)
    for load in loads:
        load.start()

    sink_val = sink[0, 0]
    q_pos = iota((BLOCK, BLOCK + 2 * WINDOW), 0)
    k_pos = iota((BLOCK, BLOCK + 2 * WINDOW), 1)

    def attend(n):
        @pl.when(n == 0)
        def _():
            for i in range(2):
                halo[2 * i].wait_recv()

        @pl.when(n == n_tp - 1)
        def _():
            for i in range(2):
                halo[2 * i + 1].wait_recv()

        start = pl.multiple_of(n * BLOCK, BLOCK)
        keys = pl.ds(start, BLOCK + 2 * WINDOW)
        scores = lax.dot_general(
            q_buf[pl.ds(start, BLOCK), :], k_buf[keys, :], (((1,), (1,)), ((), ())), preferred_element_type=F32
        ) * HEAD_DIM ** (-0.5)
        lo = jnp.where((sp == 0) & (n == 0), WINDOW, 0)
        hi = jnp.where((sp == n_sp - 1) & (n == n_tp - 1), BLOCK + WINDOW, BLOCK + 2 * WINDOW)
        inside = (k_pos >= q_pos) & (k_pos <= q_pos + 2 * WINDOW) & (k_pos >= lo) & (k_pos < hi)
        scores = jnp.where(inside, scores, NEG_BIG)
        top = jnp.maximum(jnp.max(scores, axis=1, keepdims=True), sink_val)
        terms = jnp.exp(scores - top)
        mass = jnp.sum(terms, axis=1, keepdims=True) + jnp.exp(sink_val - top)
        value = jnp.dot(terms.astype(BF), v_buf[keys, :], preferred_element_type=F32)
        return (value / mass).astype(BF)

    my_cols = pl.ds(pl.multiple_of(me * HEAD_DIM, HEAD_DIM), HEAD_DIM)

    def a2a_copy(t, n):
        return remote(
            att.at[n], by_token.at[:, my_cols], a2a_s.at[t], a2a_r.at[t], (sp, lax.div(n, 2), lax.rem(n, 2))
        )

    def attend_pair(t, carry):
        ahead, behind = lax.rem(me + t, n_tp), lax.rem(me + n_tp - t, n_tp)
        first_val, second_val = attend(ahead), attend(behind)
        att[ahead] = first_val
        att[behind] = second_val
        a2a_copy(t, ahead).start()
        a2a_copy(n_tp - t, behind).start()
        return carry

    axis_len = (n_x, n_y)
    place = (x, y)
    zq = n_z // 4

    def plane_dev(axis, step):
        at_axis = lax.rem(place[axis] + step + axis_len[axis], axis_len[axis])
        return (y * n_x + at_axis, z, c) if axis == 0 else (at_axis * n_x + x, z, c)

    def plane_region(order, wide, d, dr, hf):
        axis = order if not wide else 1 - order
        at_axis = lax.rem(place[axis] + (axis_len[axis] - d if dr == 0 else d), axis_len[axis])
        zr = pl.ds(order * 2 * zq + hf * zq, zq)
        if wide:
            if axis == 1:
                return w_proj.at[at_axis, :, zr, c, plane_rows]
            lanes = pl.ds(pl.multiple_of(lax.rem(at_axis, 2) * 128, 128), 128)
            return w_proj.at[:, lax.div(at_axis, 2), zr, c, plane_rows, lanes]
        if axis == 0:
            lanes = pl.ds(pl.multiple_of(lax.rem(at_axis, 2) * 128, 128), 128)
            return w_proj.at[y, lax.div(at_axis, 2), zr, c, plane_rows, lanes]
        return w_proj.at[at_axis, lax.div(x, 2), zr, c, plane_rows, lanes_own]

    def plane_reach(order, wide, dr, hf):
        axis = order if not wide else 1 - order
        limit = axis_len[axis] // 2
        return limit if dr == hf else limit - 1

    def plane_copy(order, wide, d, dr, hf):
        axis = order if not wide else 1 - order
        region = plane_region(order, wide, d, dr, hf)
        s_sem, r_sem = (wide_s, wide_r) if wide else (near_s, near_r)
        sem = (order, dr, d, hf)
        return remote(region, region, s_sem.at[sem], r_sem.at[sem], plane_dev(axis, 1 if dr == 0 else -1))

    def plane_send(order, wide, d, dr, hf):
        if d < plane_reach(order, wide, dr, hf):
            copy = plane_copy(order, wide, d, dr, hf)
            copy.start()
            sends.append(copy)

    def plane_wait(order, wide, d, dr, hf):
        axis = order if not wide else 1 - order
        region = plane_region(order, wide, d, dr, hf)
        s_sem, r_sem = (wide_s, wide_r) if wide else (near_s, near_r)
        sem = (order, dr, d - 1, hf)
        remote(region, region, s_sem.at[sem], r_sem.at[sem], plane_dev(axis, 1 if dr == 0 else -1)).wait_recv()

    def plane_steps(order, wide):
        limit = axis_len[order if not wide else 1 - order] // 2
        steps = []
        for d in range(1, limit + 1):
            for sub in range(2):
                for dr in range(2):
                    hf = dr if sub == 0 else 1 - dr
                    if d <= plane_reach(order, wide, dr, hf):
                        steps.append((d, dr, hf))
        return steps

    wpairs = []

    def wpair_send(region, index):
        wpairs.append(push(region, region, wpair_s.at[index], wpair_r.at[index], partner))

    def wpair_wait(order, d, dr, hf, index):
        axis = 1 - order
        at_axis = lax.rem(place[axis] + (axis_len[axis] - d if dr == 0 else d), axis_len[axis])
        zr = pl.ds(order * 2 * zq + hf * zq, zq)
        if axis == 1:
            region = w_proj.at[at_axis, :, zr, 1 - c, plane_rows]
        else:
            lanes = pl.ds(pl.multiple_of(lax.rem(at_axis, 2) * 128, 128), 128)
            region = w_proj.at[:, lax.div(at_axis, 2), zr, 1 - c, plane_rows, lanes]
        remote(region, region, wpair_s.at[index], wpair_r.at[index], partner).wait_recv()

    split = max(1, (n_tp // 2) // 2)
    lax.fori_loop(1, 1 + split, attend_pair, 0)
    for d in column:
        remote(w_own, col_region(d), col_s.at[d], col_r.at[d], ring_dev[0]).wait_recv()
    for hf_step in range(2):
        for order in range(2):
            for dr in range(2):
                plane_send(order, False, 0, dr, dr if hf_step == 0 else 1 - dr)
    middle = min(3 + split, n_tp // 2)
    lax.fori_loop(1 + split, middle, attend_pair, 0)

    def near_steps(low, high):
        for d, dr, hf in plane_steps(0, False):
            if low <= d < high:
                for order in range(2):
                    plane_wait(order, False, d, dr, hf)
                    plane_send(order, False, d, dr, hf)

    zrow_step(1)
    near_steps(1, 2)
    lax.fori_loop(middle, n_tp // 2, attend_pair, 0)
    opposite = lax.rem(me + n_tp // 2, n_tp)
    first_val, own_val = attend(opposite), attend(me)
    att[opposite] = first_val
    by_token[:, my_cols] = own_val
    a2a_copy(n_tp // 2, opposite).start()
    near_steps(2, n_sp)
    for hf_step in range(2):
        for order in range(2):
            for dr in range(2):
                plane_send(order, True, 0, dr, dr if hf_step == 0 else 1 - dr)
    for order in range(2):
        for hf in range(2):
            wpair_send(plane_region(order, True, 0, 0, hf), (order, hf, 0))
    zrow_step(2)

    ahead = route_group[...] - sp
    ahead = jnp.where(ahead < 0, ahead + n_sp, ahead)
    chosen = iota((n_sp, tok), 0) == ahead
    earlier = one_hot(iota((tok, tok), 0) < iota((tok, tok), 1))
    ranks = jnp.dot(one_hot(chosen), earlier, preferred_element_type=F32)
    rank = jnp.sum(jnp.where(chosen, ranks, 0.0), axis=0, keepdims=True).astype(jnp.int32)
    slot_row = iota((n_sp * SLOT, tok), 0)
    placing[...] = one_hot(slot_row == ahead * SLOT + rank)
    in_half = jnp.where(ahead >= half, ahead - half, ahead)
    lane_hot = one_hot(iota((128, tok), 0) == in_half * cap + rank)
    gate_at = jnp.zeros((n_sp * SLOT, tok), F32)
    for k in range(2):
        member = route_member[k : k + 1, :]
        weight = route_weight[k : k + 1, :].astype(F32)
        gate_at = gate_at + jnp.where(slot_row == ahead * SLOT + cap + member, weight, 0.0)
    gate_rows[...] = lax.dot_general(
        gate_at.astype(BF), lane_hot, (((1,), (1,)), ((), ())), preferred_element_type=F32
    )

    def zrow_all(core):
        region = w_proj.at[:, :, :, core, ring_rows, :]
        return remote(region, region, zpair_s.at[0], zpair_r.at[0], partner)

    wide_steps = plane_steps(0, True)
    for i, step in enumerate(wide_steps):
        if i == len(wide_steps) // 3:
            for d in range(3, far):
                zrow_step(d)
        if i == len(wide_steps) * 2 // 3:
            if far > 2:
                zrow_step(far)
            zrow_all(c).start()
        for order in range(2):
            d, dr, hf = step
            plane_wait(order, True, d, dr, hf)
            plane_send(order, True, d, dr, hf)
            index = (order, hf, 1 + (d - 1) * 2 + dr)
            wpair_send(plane_region(order, True, d, dr, hf), index)
    for t in range(1, n_tp):
        source = pl.ds(pl.multiple_of(lax.rem(me + n_tp - t, n_tp) * HEAD_DIM, HEAD_DIM), HEAD_DIM)
        remote(att.at[0], by_token.at[:, source], a2a_s.at[t], a2a_r.at[t], partner).wait_recv()
    for order in range(2):
        for hf in range(2):
            wpair_wait(order, 0, 0, hf, (order, hf, 0))
    for d, dr, hf in plane_steps(0, True):
        for order in range(2):
            wpair_wait(order, d, dr, hf, (order, hf, 1 + (d - 1) * 2 + dr))

    zrow_all(1 - c).wait_recv()
    w_tiles = width // tile

    def project(i, carry):
        block = w_proj[lax.div(i, w_tiles // n_y), lax.rem(i, w_tiles // n_y)].reshape(n_tp * HEAD_DIM, tile)
        columns = pl.ds(pl.multiple_of(i * tile, tile), tile)
        proj[:, columns] = jnp.dot(by_token[...], block, preferred_element_type=F32)
        return carry

    lax.fori_loop(0, w_tiles, project, 0)

    def norms(i, carry):
        at_rows = pl.ds(pl.multiple_of(i * 16, 16), 16)
        value = proj[at_rows, :]
        scale = lax.rsqrt(jnp.mean(value * value, axis=1, keepdims=True) + EPS)
        mixed_bf = (residual[at_rows, :].astype(F32) + mixer_gain[...] * (value * scale)).astype(BF)
        mixed[at_rows, :] = mixed_bf
        mixed_f = mixed_bf.astype(F32)
        scale = lax.rsqrt(jnp.mean(mixed_f * mixed_f, axis=1, keepdims=True) + EPS)
        normed[at_rows, :] = (mixed_f * scale * expert_gain[...]).astype(BF)
        return carry

    lax.fori_loop(0, tok // 16, norms, 0)

    head = jnp.dot(placing[...], normed[:, 0:128], preferred_element_type=F32)
    send[:, 0:128] = (head + gate_rows[...]).astype(BF)
    send[:, 128:] = jnp.dot(placing[...], normed[:, 128:], preferred_element_type=F32).astype(BF)
    def cut(ch):
        return pl.ds(ch * span, span)

    disp = {}
    for hf in range(2):
        for ch in range(CHUNKS):
            for j in range(hf * half, (hf + 1) * half):
                at_slot = (pl.ds(j * SLOT, SLOT), cut(ch))
                if j > 0:
                    disp[(ch, j)] = push(
                        send.at[at_slot],
                        arr.at[at_slot],
                        disp_s.at[ch, j],
                        disp_r.at[ch, j],
                        (lax.rem(sp + j, n_sp), z, c),
                    )
    arr[0:SLOT] = send[0:SLOT]

    def reach(dr, hf):
        return far if dr == hf else far - 1

    def at(dr, d):
        return (n_z - d) % n_z if dr == 0 else d

    arrivals = [(1, 0), (1, 1)] + [(d, 0) for d in range(2, far + 1)] + [(d, 1) for d in range(2, far)]
    together = [[(0, 0), (0, 1)]]
    for d, kind in arrivals:
        together.append([(at(dr, d), kind if d == 1 or dr == 0 else 1 - kind) for dr in range(2)])
    place_at = {unit: (i, sub) for i, units in enumerate(together) for sub, unit in enumerate(units)}

    def spot(o, rc, hf):
        i, sub = place_at[(o, hf)]
        return i, pl.ds((sub * 2 + rc) * hr, hr)

    def sum_spot(o, hf):
        i, sub = place_at[(o, hf)]
        return i, pl.ds(sub * hr, hr)

    ring = {}
    ring_g = {}
    pair = {}

    def ring_send(dr, d, hf, ch):
        src, dst = at(dr, d), at(dr, d + 1)
        sem = (dr, d, hf, ch)
        ring[sem] = push(
            rows.at[(*spot(src, 0, hf), cut(ch))],
            rows.at[(*spot(dst, 0, hf), cut(ch))],
            ring_s.at[sem],
            ring_r.at[sem],
            ring_dev[dr],
        )
        if ch == 0:
            sem = (dr, d, hf)
            ring_g[sem] = push(
                gates.at[src, 0, hf], gates.at[dst, 0, hf], rgate_s.at[sem], rgate_r.at[sem], ring_dev[dr]
            )

    def ring_wait(dr, d, hf, ch):
        ring[(dr, d - 1, hf, ch)].wait_recv()
        if ch == 0:
            ring_g[(dr, d - 1, hf)].wait_recv()

    def pair_send(o, hf):
        pair[(o, hf)] = (
            push(rows.at[spot(o, 0, hf)], rows.at[spot(o, 1, hf)], pair_s.at[o, hf], pair_r.at[o, hf], partner),
            push(gates.at[o, 0, hf], gates.at[o, 1, hf], pgate_s.at[o, hf], pgate_r.at[o, hf], partner),
        )

    for hf in range(2):
        block = pl.ds(hf * half * SLOT, half * SLOT)
        for ch in range(CHUNKS):
            for j in range(hf * half, (hf + 1) * half):
                if j > 0:
                    disp[(ch, j)].wait_recv()
            if ch == 0:
                gates[0, 0, hf] = jnp.dot(
                    gate_pick[...], arr[block, 0:128], preferred_element_type=F32
                ).astype(BF)
            rows[(*spot(0, 0, hf), cut(ch))] = jnp.dot(
                pick[...], arr[block, cut(ch)], preferred_element_type=F32
            ).astype(BF)
            ring_send(0, 0, hf, ch)
            ring_send(1, 0, hf, ch)
        pair_send(0, hf)

    for load in loads:
        load.wait()

    eye = one_hot(iota((hr, 128), 0) == iota((hr, 128), 1))
    summed = {}

    def compute(step):
        for sub, (o, hf) in enumerate(together[step]):
            for copy in pair[(o, hf)]:
                copy.wait_recv()
            for rc in range(2):
                gcol[pl.ds((sub * 2 + rc) * hr, hr)] = lax.dot_general(
                    eye, gates[o, rc, hf], (((1,), (1,)), ((), ())), preferred_element_type=F32
                )
        for e in range(experts):
            pre = jnp.dot(rows[step], w_in[e], preferred_element_type=F32)
            gate_pre, up_pre = pre[:, :hid], pre[:, hid:]
            scaled = gate_pre / (1.0 + jnp.exp(-gate_pre)) * up_pre * gcol[:, e : e + 1]
            hidden[:, e * hid : (e + 1) * hid] = scaled.astype(BF)

        def down(i, carry):
            columns = pl.ds(pl.multiple_of(i * tile, tile), tile)
            piece = jnp.dot(hidden[...], w_out[:, columns], preferred_element_type=F32).astype(BF)
            for sub in range(2):
                own[step, pl.ds(sub * hr, hr), columns] = piece[sub * 2 * hr : (sub * 2 + 1) * hr]
                oth[step, pl.ds(sub * hr, hr), columns] = piece[(sub * 2 + 1) * hr : (sub * 2 + 2) * hr]
            return carry

        lax.fori_loop(0, width // tile, down, 0)
        summed[step] = push(oth.at[step], got.at[step], sum_s.at[step], sum_r.at[step], partner)

    hops = {}
    settled = set()

    def settle(o, hf):
        step = place_at[(o, hf)][0]
        if step not in settled:
            summed[step].wait_recv()
            settled.add(step)

    def own_rows(o, hf, i):
        step, sub = place_at[(o, hf)]
        return step, pl.ds(pl.multiple_of(sub * hr + i * 16, 16), 16)

    def hop_send(dr, d, hf, ch):
        o = (n_z - d) % n_z if dr == 1 else d
        settle(o, hf)
        start = d == reach(1 - dr, hf)
        if start:
            src = own.at[(*sum_spot(o, hf), cut(ch))]
        else:
            hops[(dr, d + 1, hf, ch)].wait_recv()
            src = hop.at[dr, d, hf, :, cut(ch)]

        def add(i, carry):
            local = pl.ds(pl.multiple_of(i * 16, 16), 16)
            at_rows = (*own_rows(o, hf, i), cut(ch))
            total = own[at_rows].astype(F32) + got[at_rows].astype(F32)
            if not start:
                total = total + hop[dr, d, hf, local, cut(ch)].astype(F32)
            src[local] = total.astype(BF)
            return carry

        lax.fori_loop(0, hr // 16, add, 0)
        sem = (dr, d, hf, ch)
        hops[sem] = push(src, hop.at[dr, d - 1, hf, :, cut(ch)], hop_s.at[sem], hop_r.at[sem], ring_dev[dr])

    returned = {}

    def finish(ch):
        for hf in range(2):
            settle(0, hf)
            for dr in range(2):
                hops[(dr, 1, hf, ch)].wait_recv()

            def last_add(i, carry):
                local = pl.ds(pl.multiple_of(i * 16, 16), 16)
                at_rows = (*own_rows(0, hf, i), cut(ch))
                total = own[at_rows].astype(F32) + got[at_rows].astype(F32)
                total = total + (
                    hop[0, 0, hf, local, cut(ch)].astype(F32) + hop[1, 0, hf, local, cut(ch)].astype(F32)
                )
                own[at_rows] = total.astype(BF)
                return carry

            lax.fori_loop(0, hr // 16, last_add, 0)
            ret[pl.ds(hf * half * SLOT, half * SLOT), cut(ch)] = jnp.dot(
                pick_t[...], own[(*sum_spot(0, hf), cut(ch))], preferred_element_type=F32
            ).astype(BF)
            for j in range(hf * half, (hf + 1) * half):
                at_slot = (pl.ds(j * SLOT, SLOT), cut(ch))
                if j == 0:
                    back[0:SLOT, cut(ch)] = ret[0:SLOT, cut(ch)]
                else:
                    returned[(ch, j)] = push(
                        ret.at[at_slot],
                        back.at[at_slot],
                        ret_s.at[ch, j],
                        ret_r.at[ch, j],
                        (lax.rem(sp + n_sp - j, n_sp), z, c),
                    )

    compute(0)

    def long_hop(d, ch):
        for dr in range(2):
            hop_send(dr, d, 1 - dr, ch)

    done = {0}

    def need(step):
        if step not in done:
            compute(step)
            done.add(step)

    far_step = place_at[(far, 0)][0]
    for k, (d, kind) in enumerate(arrivals):
        step = k + 1
        for ch in range(CHUNKS):
            if step == far_step + 1 and ch == CHUNKS // 2:
                need(far_step)
            for dr in range(2):
                hf = together[step][dr][1]
                ring_wait(dr, d, hf, ch)
                if d < reach(dr, hf) and not (d == 1 and dr != hf):
                    ring_send(dr, d, hf, ch)
        if (d, kind) == (far - 1, 0):
            for ch in range(CHUNKS):
                for dr in range(2):
                    if 1 < reach(dr, 1 - dr):
                        ring_send(dr, 1, 1 - dr, ch)
        for o, hf in together[step]:
            pair_send(o, hf)
        if k > 0 and step != far_step + 1 and step != len(arrivals):
            need(step - 1)
        if step == len(arrivals) - 1 and far > 2:
            for ch in range(CHUNKS):
                long_hop(far, ch)
            need(step)
    if far == 2:
        need(1)
        need(2)
        need(3)
        for ch in range(CHUNKS):
            long_hop(far, ch)
    for ch in range(CHUNKS // 2):
        long_hop(far - 1, ch)
    need(len(arrivals))
    for ch in range(CHUNKS // 2, CHUNKS):
        long_hop(far - 1, ch)
    events = []
    for ch in range(CHUNKS):
        at_key = 1.2 * ch
        for d in range(far - 1, 0, -1):
            events.append((at_key, ch, d, 1))
            at_key += 1
            if d > 1:
                events.append((at_key, ch, d - 1, 0))
                at_key += 1
        events.append((at_key + 0.3, ch, 0, 0))
    for _, ch, d, kind in sorted(events):
        if d == 0:
            finish(ch)
        else:
            for dr in range(2):
                hop_send(dr, d, 1 - dr if kind == 0 else dr, ch)
    eye_tok = one_hot(iota((tok, tok), 0) == iota((tok, tok), 1))
    placing_t = lax.dot_general(
        eye_tok, placing[...], (((1,), (1,)), ((), ())), preferred_element_type=F32
    ).astype(BF)
    for ch in range(CHUNKS):
        for j in range(1, n_sp):
            returned[(ch, j)].wait_recv()
        expert_out = jnp.dot(placing_t, back[:, cut(ch)], preferred_element_type=F32)
        out[:, cut(ch)] = (mixed[:, cut(ch)].astype(F32) + expert_out).astype(BF)
    for t in range(1, n_tp):
        a2a_copy(t, lax.rem(me + t, n_tp)).wait_send()
    zrow_all(c).wait_send()
    for copy in sends:
        copy.wait_send()


def per_device(
    queries,
    key_heads,
    value_heads,
    sink_logit,
    out_weight,
    residual,
    mixer_gain,
    expert_gain,
    route_group,
    route_member,
    route_weight,
    gate_weight,
    up_weight,
    down_weight,
    n_x=4,
    cap=GROUP_CAP,
    kv_share=HEADS // KV_HEADS,
):
    n_sp, n_z = lax.axis_size("sp"), lax.axis_size("tp_0")
    n_y = n_sp // n_x
    n_tp = 2 * n_z
    tok, width = residual.shape
    seq = queries.shape[0]
    experts, hid = down_weight.shape[0], down_weight.shape[1]
    half = n_sp // 2
    hr = half * cap
    far = n_z // 2
    r = np.arange(hr)
    padded = r // cap * SLOT + r % cap
    i = np.arange(half * SLOT)
    e = np.arange(16)
    pick = jnp.asarray(i[None, :] == padded[:, None], BF)
    pick_t = jnp.asarray(i[:, None] == padded[None, :], BF)
    gate_pick = jnp.asarray((i[None, :] % SLOT == e[:, None] + cap) & (e[:, None] < experts), BF)
    vmem = pl.BlockSpec(memory_space=pltpu.VMEM)
    anywhere = pl.BlockSpec(memory_space=pl.ANY)
    dma = pltpu.SemaphoreType.DMA
    bf_bufs = [
        (seq, HEAD_DIM),
        (seq + 2 * WINDOW, HEAD_DIM),
        (seq + 2 * WINDOW, HEAD_DIM),
        (n_tp, BLOCK, HEAD_DIM),
        (tok, n_tp * HEAD_DIM),
        (n_y, n_x // 2, n_z, 2, 128, 256),
        None,
        (tok, width),
        (tok, width),
        (n_sp * SLOT, tok),
        None,
        (n_sp * SLOT, width),
        (n_sp * SLOT, width),
        (n_z, 4 * hr, width),
        (n_z, 2, 2, 16, 128),
        None,
        (4 * hr, experts * hid),
        (experts, width, 2 * hid),
        (experts * hid, width),
        (n_z, 2 * hr, width),
        (n_z, 2 * hr, width),
        (n_z, 2 * hr, width),
        (2, far, 2, hr, width),
        (n_sp * SLOT, width),
        (n_sp * SLOT, width),
    ]
    f32_bufs = iter([(tok, width), (n_sp * SLOT, 128), (4 * hr, 16)])
    buffers = [pltpu.VMEM(s, BF) if s is not None else pltpu.VMEM(next(f32_bufs), F32) for s in bf_bufs]
    sems = [(4,)]
    sems += [(2, 2)] * 2 + [(n_tp,)] * 2 + [(n_z,)] * 2 + [(2, 2, 2, 2)] * 4 + [(2, 2, 5)] * 2
    sems += [(2, far, 2)] * 2 + [(1,)] * 2 + [(width // 256,)]
    sems += [(experts, 3)] + [(CHUNKS, n_sp)] * 2 + [(2, far, 2, CHUNKS)] * 2 + [(2, far, 2)] * 2 + [(n_z, 2)] * 4 + [(n_z,)] * 2
    sems += [(2, far + 1, 2, CHUNKS)] * 2 + [(CHUNKS, n_sp)] * 2
    return pl.pallas_call(
        functools.partial(layer_kernel, n_sp, n_x, n_z, kv_share, cap),
        out_shape=jax.ShapeDtypeStruct((tok, width), BF),
        in_specs=[anywhere] * 3 + [vmem, anywhere] + [vmem] * 9 + [anywhere] * 3,
        out_specs=vmem,
        scratch_shapes=buffers + [dma(s) for s in sems],
        compiler_params=pltpu.CompilerParams(
            collective_id=0, has_side_effects=True, vmem_limit_bytes=VMEM_LIMIT
        ),
    )(
        queries,
        key_heads,
        value_heads,
        sink_logit.reshape(1, 1),
        out_weight,
        residual,
        mixer_gain.reshape(1, -1),
        expert_gain.reshape(1, -1),
        route_group.reshape(1, -1),
        route_member.T,
        route_weight.T,
        pick,
        pick_t,
        gate_pick,
        gate_weight,
        up_weight,
        down_weight,
    )


def solution(mesh):
    torus = Mesh(mesh.devices.reshape(mesh.shape["sp"], 8, 2), ("sp", "tp_0", "tp_1"))
    placed = (
        P("sp", TP),
        P("sp", None),
        P("sp", None),
        P(TP),
        P(TP, None),
        P(SP_TP, None),
        P(),
        P(),
        P(SP_TP),
        P(SP_TP, None),
        P(SP_TP, None),
        P("sp", None, TP),
        P("sp", None, TP),
        P("sp", TP, None),
    )
    return jax.shard_map(
        per_device, mesh=torus, in_specs=placed, out_specs=P(SP_TP, None), check_vma=False
    )
```

```python
import functools

import jax
import jax.numpy as jnp
import numpy as np
from jax import lax
from jax.experimental import pallas as pl
from jax.experimental.pallas import tpu as pltpu
from jax.sharding import Mesh
from jax.sharding import PartitionSpec as P

HEADS = 16
KV_HEADS = 4
HEAD_DIM = 128
WINDOW = 128
BLOCK = 128
GROUP_EXPERTS = 3
GROUP_CAP = 10
SLOT = 16
CHUNKS = 4
Z_ROWS = 32
TP = ("tp_0", "tp_1")
SP_TP = ("sp", "tp_0", "tp_1")
MESH_ID = pl.DeviceIdType.MESH
VMEM_LIMIT = 62 * 1024 * 1024

EPS = 1e-06
NEG_BIG = -1e30
BF = jnp.bfloat16
F32 = jnp.float32


def one_hot(condition):
    return jnp.where(condition, 1.0, 0.0).astype(BF)


def iota(shape, dim):
    return lax.broadcasted_iota(jnp.int32, shape, dim)


def layer_kernel(
    n_sp,
    n_x,
    n_z,
    kv_share,
    cap,
    queries,
    key_heads,
    value_heads,
    sink,
    out_weight,
    residual,
    mixer_gain,
    expert_gain,
    route_group,
    route_member,
    route_weight,
    pick,
    pick_t,
    gate_pick,
    wg,
    wu,
    wd,
    out,
    q_buf,
    k_buf,
    v_buf,
    att,
    by_token,
    w_proj,
    proj,
    normed,
    mixed,
    placing,
    gate_rows,
    send,
    arr,
    rows,
    gates,
    gcol,
    hidden,
    w_in,
    w_out,
    own,
    oth,
    got,
    hop,
    ret,
    back,
    load_sem,
    halo_s,
    halo_r,
    a2a_s,
    a2a_r,
    col_s,
    col_r,
    near_s,
    near_r,
    wide_s,
    wide_r,
    wpair_s,
    wpair_r,
    zrow_s,
    zrow_r,
    zpair_s,
    zpair_r,
    zload_sem,
    w_sem,
    disp_s,
    disp_r,
    ring_s,
    ring_r,
    rgate_s,
    rgate_r,
    pair_s,
    pair_r,
    pgate_s,
    pgate_r,
    sum_s,
    sum_r,
    hop_s,
    hop_r,
    ret_s,
    ret_r,
):
    sp, z, c = lax.axis_index("sp"), lax.axis_index("tp_0"), lax.axis_index("tp_1")
    me = z * 2 + c
    n_tp = 2 * n_z
    y, x = lax.div(sp, n_x), lax.rem(sp, n_x)
    n_y = n_sp // n_x
    tok, width = residual.shape
    experts, hid = wd.shape[0], wd.shape[1]
    half = n_sp // 2
    hr = half * cap
    far = n_z // 2
    tile = 256
    span = width // CHUNKS
    sends = []

    def remote(src, dst, s_sem, r_sem, dev):
        return pltpu.make_async_remote_copy(
            src_ref=src, dst_ref=dst, send_sem=s_sem, recv_sem=r_sem, device_id=dev, device_id_type=MESH_ID
        )

    def push(src, dst, s_sem, r_sem, dev):
        copy = remote(src, dst, s_sem, r_sem, dev)
        copy.start()
        sends.append(copy)
        return copy

    partner = (sp, z, 1 - c)
    ring_dev = ((sp, lax.rem(z + 1, n_z), c), (sp, lax.rem(z + n_z - 1, n_z), c))

    seq = q_buf.shape[0]
    head_at = pl.ds(pl.multiple_of(lax.div(me, kv_share) * HEAD_DIM, HEAD_DIM), HEAD_DIM)
    inner = pl.ds(WINDOW, seq)
    col_own = pl.ds(pl.multiple_of(sp * 128, 128), 128)
    lanes_own = pl.ds(pl.multiple_of(lax.rem(x, 2) * 128, 128), 128)
    plane_rows = pl.ds(Z_ROWS, HEAD_DIM - Z_ROWS)
    ring_rows = pl.ds(0, Z_ROWS)
    w_own = w_proj.at[y, lax.div(x, 2), z, c, plane_rows, lanes_own]
    first = [
        pltpu.make_async_copy(key_heads.at[:, head_at], k_buf.at[inner], load_sem.at[0]),
        pltpu.make_async_copy(value_heads.at[:, head_at], v_buf.at[inner], load_sem.at[1]),
        pltpu.make_async_copy(out_weight.at[plane_rows, col_own], w_own, load_sem.at[2]),
        pltpu.make_async_copy(queries, q_buf, load_sem.at[3]),
    ]
    for i in range(width // tile):
        per_y = width // tile // n_y
        first.append(
            pltpu.make_async_copy(
                out_weight.at[ring_rows, pl.ds(i * tile, tile)],
                w_proj.at[i // per_y, i % per_y, z, c, ring_rows, :],
                zload_sem.at[i],
            )
        )
    for load in first:
        load.start()
    loads = []
    for e in range(experts):
        loads.append(pltpu.make_async_copy(wg.at[e], w_in.at[e, :, pl.ds(0, hid)], w_sem.at[e, 0]))
        loads.append(pltpu.make_async_copy(wu.at[e], w_in.at[e, :, pl.ds(hid, hid)], w_sem.at[e, 1]))
        loads.append(pltpu.make_async_copy(wd.at[e], w_out.at[pl.ds(e * hid, hid), :], w_sem.at[e, 2]))

    barrier = pltpu.get_barrier_semaphore()
    for j in range(1, n_sp):
        pl.semaphore_signal(barrier, inc=1, device_id=(lax.rem(sp + j, n_sp), z, c), device_id_type=MESH_ID)
    for j in range(1, n_tp):
        n = lax.rem(me + j, n_tp)
        pl.semaphore_signal(
            barrier, inc=1, device_id=(sp, lax.div(n, 2), lax.rem(n, 2)), device_id_type=MESH_ID
        )
    for load in first:
        load.wait()
    pl.semaphore_wait(barrier, n_sp - 1 + n_tp - 1)

    after, before = lax.rem(sp + 1, n_sp), lax.rem(sp + n_sp - 1, n_sp)
    low, high = pl.ds(0, WINDOW), pl.ds(WINDOW + seq, WINDOW)
    halo = []
    for i, buf in enumerate((k_buf, v_buf)):
        halo.append(push(buf.at[pl.ds(seq, WINDOW)], buf.at[low], halo_s.at[0, i], halo_r.at[0, i], (after, z, c)))
        halo.append(push(buf.at[pl.ds(WINDOW, WINDOW)], buf.at[high], halo_s.at[1, i], halo_r.at[1, i], (before, z, c)))

    def col_region(d):
        return w_proj.at[y, lax.div(x, 2), lax.rem(z + n_z - d, n_z), c, plane_rows, lanes_own]

    column = []
    for k in range(1, n_z):
        d = (k + 1) // 2 if k % 2 else n_z - k // 2
        push(w_own, w_own, col_s.at[d], col_r.at[d], (sp, lax.rem(z + d, n_z), c))
        column.append(d)
    def zrow_reach(dr, hf):
        return far if dr == hf else far - 1

    def zrow_region(dr, d, hf):
        at_z = lax.rem(z + (n_z - d if dr == 0 else d), n_z)
        return w_proj.at[pl.ds(hf * (n_y // 2), n_y // 2), :, at_z, c, ring_rows, :]

    def zrow_step(d):
        for sub in range(2):
            for dr in range(2):
                hf = dr if sub == 0 else 1 - dr
                region = zrow_region(dr, d, hf)
                if 0 < d <= zrow_reach(dr, hf):
                    sem = (dr, d - 1, hf)
                    remote(region, region, zrow_s.at[sem], zrow_r.at[sem], ring_dev[dr]).wait_recv()
                if d < zrow_reach(dr, hf):
                    sem = (dr, d, hf)
                    push(region, region, zrow_s.at[sem], zrow_r.at[sem], ring_dev[dr])

    zrow_step(0)
    for load in loads:
        load.start()

    sink_val = sink[0, 0]
    q_pos = iota((BLOCK, BLOCK + 2 * WINDOW), 0)
    k_pos = iota((BLOCK, BLOCK + 2 * WINDOW), 1)

    def attend(n):
        @pl.when(n == 0)
        def _():
            for i in range(2):
                halo[2 * i].wait_recv()

        @pl.when(n == n_tp - 1)
        def _():
            for i in range(2):
                halo[2 * i + 1].wait_recv()

        start = pl.multiple_of(n * BLOCK, BLOCK)
        keys = pl.ds(start, BLOCK + 2 * WINDOW)
        scores = lax.dot_general(
            q_buf[pl.ds(start, BLOCK), :], k_buf[keys, :], (((1,), (1,)), ((), ())), preferred_element_type=F32
        ) * HEAD_DIM ** (-0.5)
        lo = jnp.where((sp == 0) & (n == 0), WINDOW, 0)
        hi = jnp.where((sp == n_sp - 1) & (n == n_tp - 1), BLOCK + WINDOW, BLOCK + 2 * WINDOW)
        inside = (k_pos >= q_pos) & (k_pos <= q_pos + 2 * WINDOW) & (k_pos >= lo) & (k_pos < hi)
        scores = jnp.where(inside, scores, NEG_BIG)
        top = jnp.maximum(jnp.max(scores, axis=1, keepdims=True), sink_val)
        terms = jnp.exp(scores - top)
        mass = jnp.sum(terms, axis=1, keepdims=True) + jnp.exp(sink_val - top)
        value = jnp.dot(terms.astype(BF), v_buf[keys, :], preferred_element_type=F32)
        return (value / mass).astype(BF)

    my_cols = pl.ds(pl.multiple_of(me * HEAD_DIM, HEAD_DIM), HEAD_DIM)

    def a2a_copy(t, n):
        return remote(
            att.at[n], by_token.at[:, my_cols], a2a_s.at[t], a2a_r.at[t], (sp, lax.div(n, 2), lax.rem(n, 2))
        )

    def attend_pair(t, carry):
        ahead, behind = lax.rem(me + t, n_tp), lax.rem(me + n_tp - t, n_tp)
        first_val, second_val = attend(ahead), attend(behind)
        att[ahead] = first_val
        att[behind] = second_val
        a2a_copy(t, ahead).start()
        a2a_copy(n_tp - t, behind).start()
        return carry

    axis_len = (n_x, n_y)
    place = (x, y)
    zq = n_z // 4

    def plane_dev(axis, step):
        at_axis = lax.rem(place[axis] + step + axis_len[axis], axis_len[axis])
        return (y * n_x + at_axis, z, c) if axis == 0 else (at_axis * n_x + x, z, c)

    def plane_region(order, wide, d, dr, hf):
        axis = order if not wide else 1 - order
        at_axis = lax.rem(place[axis] + (axis_len[axis] - d if dr == 0 else d), axis_len[axis])
        zr = pl.ds(order * 2 * zq + hf * zq, zq)
        if wide:
            if axis == 1:
                return w_proj.at[at_axis, :, zr, c, plane_rows]
            lanes = pl.ds(pl.multiple_of(lax.rem(at_axis, 2) * 128, 128), 128)
            return w_proj.at[:, lax.div(at_axis, 2), zr, c, plane_rows, lanes]
        if axis == 0:
            lanes = pl.ds(pl.multiple_of(lax.rem(at_axis, 2) * 128, 128), 128)
            return w_proj.at[y, lax.div(at_axis, 2), zr, c, plane_rows, lanes]
        return w_proj.at[at_axis, lax.div(x, 2), zr, c, plane_rows, lanes_own]

    def plane_reach(order, wide, dr, hf):
        axis = order if not wide else 1 - order
        limit = axis_len[axis] // 2
        return limit if dr == hf else limit - 1

    def plane_copy(order, wide, d, dr, hf):
        axis = order if not wide else 1 - order
        region = plane_region(order, wide, d, dr, hf)
        s_sem, r_sem = (wide_s, wide_r) if wide else (near_s, near_r)
        sem = (order, dr, d, hf)
        return remote(region, region, s_sem.at[sem], r_sem.at[sem], plane_dev(axis, 1 if dr == 0 else -1))

    def plane_send(order, wide, d, dr, hf):
        if d < plane_reach(order, wide, dr, hf):
            copy = plane_copy(order, wide, d, dr, hf)
            copy.start()
            sends.append(copy)

    def plane_wait(order, wide, d, dr, hf):
        axis = order if not wide else 1 - order
        region = plane_region(order, wide, d, dr, hf)
        s_sem, r_sem = (wide_s, wide_r) if wide else (near_s, near_r)
        sem = (order, dr, d - 1, hf)
        remote(region, region, s_sem.at[sem], r_sem.at[sem], plane_dev(axis, 1 if dr == 0 else -1)).wait_recv()

    def plane_steps(order, wide):
        limit = axis_len[order if not wide else 1 - order] // 2
        steps = []
        for d in range(1, limit + 1):
            for sub in range(2):
                for dr in range(2):
                    hf = dr if sub == 0 else 1 - dr
                    if d <= plane_reach(order, wide, dr, hf):
                        steps.append((d, dr, hf))
        return steps

    wpairs = []

    def wpair_send(region, index):
        wpairs.append(push(region, region, wpair_s.at[index], wpair_r.at[index], partner))

    def wpair_wait(order, d, dr, hf, index):
        axis = 1 - order
        at_axis = lax.rem(place[axis] + (axis_len[axis] - d if dr == 0 else d), axis_len[axis])
        zr = pl.ds(order * 2 * zq + hf * zq, zq)
        if axis == 1:
            region = w_proj.at[at_axis, :, zr, 1 - c, plane_rows]
        else:
            lanes = pl.ds(pl.multiple_of(lax.rem(at_axis, 2) * 128, 128), 128)
            region = w_proj.at[:, lax.div(at_axis, 2), zr, 1 - c, plane_rows, lanes]
        remote(region, region, wpair_s.at[index], wpair_r.at[index], partner).wait_recv()

    split = max(1, (n_tp // 2) // 2)
    lax.fori_loop(1, 1 + split, attend_pair, 0)
    for d in column:
        remote(w_own, col_region(d), col_s.at[d], col_r.at[d], ring_dev[0]).wait_recv()
    for hf_step in range(2):
        for order in range(2):
            for dr in range(2):
                plane_send(order, False, 0, dr, dr if hf_step == 0 else 1 - dr)
    middle = min(3 + split, n_tp // 2)
    lax.fori_loop(1 + split, middle, attend_pair, 0)

    def near_steps(low, high):
        for d, dr, hf in plane_steps(0, False):
            if low <= d < high:
                for order in range(2):
                    plane_wait(order, False, d, dr, hf)
                    plane_send(order, False, d, dr, hf)

    zrow_step(1)
    near_steps(1, 2)
    lax.fori_loop(middle, n_tp // 2, attend_pair, 0)
    opposite = lax.rem(me + n_tp // 2, n_tp)
    first_val, own_val = attend(opposite), attend(me)
    att[opposite] = first_val
    by_token[:, my_cols] = own_val
    a2a_copy(n_tp // 2, opposite).start()
    near_steps(2, n_sp)
    for hf_step in range(2):
        for order in range(2):
            for dr in range(2):
                plane_send(order, True, 0, dr, dr if hf_step == 0 else 1 - dr)
    for order in range(2):
        for hf in range(2):
            wpair_send(plane_region(order, True, 0, 0, hf), (order, hf, 0))
    zrow_step(2)

    ahead = route_group[...] - sp
    ahead = jnp.where(ahead < 0, ahead + n_sp, ahead)
    chosen = iota((n_sp, tok), 0) == ahead
    earlier = one_hot(iota((tok, tok), 0) < iota((tok, tok), 1))
    ranks = jnp.dot(one_hot(chosen), earlier, preferred_element_type=F32)
    rank = jnp.sum(jnp.where(chosen, ranks, 0.0), axis=0, keepdims=True).astype(jnp.int32)
    slot_row = iota((n_sp * SLOT, tok), 0)
    placing[...] = one_hot(slot_row == ahead * SLOT + rank)
    in_half = jnp.where(ahead >= half, ahead - half, ahead)
    lane_hot = one_hot(iota((128, tok), 0) == in_half * cap + rank)
    gate_at = jnp.zeros((n_sp * SLOT, tok), F32)
    for k in range(2):
        member = route_member[k : k + 1, :]
        weight = route_weight[k : k + 1, :].astype(F32)
        gate_at = gate_at + jnp.where(slot_row == ahead * SLOT + cap + member, weight, 0.0)
    gate_rows[...] = lax.dot_general(
        gate_at.astype(BF), lane_hot, (((1,), (1,)), ((), ())), preferred_element_type=F32
    )

    def zrow_all(core):
        region = w_proj.at[:, :, :, core, ring_rows, :]
        return remote(region, region, zpair_s.at[0], zpair_r.at[0], partner)

    wide_steps = plane_steps(0, True)
    for i, step in enumerate(wide_steps):
        if i == len(wide_steps) // 3:
            for d in range(3, far):
                zrow_step(d)
        if i == len(wide_steps) * 2 // 3:
            if far > 2:
                zrow_step(far)
            zrow_all(c).start()
        for order in range(2):
            d, dr, hf = step
            plane_wait(order, True, d, dr, hf)
            plane_send(order, True, d, dr, hf)
            index = (order, hf, 1 + (d - 1) * 2 + dr)
            wpair_send(plane_region(order, True, d, dr, hf), index)
    for t in range(1, n_tp):
        source = pl.ds(pl.multiple_of(lax.rem(me + n_tp - t, n_tp) * HEAD_DIM, HEAD_DIM), HEAD_DIM)
        remote(att.at[0], by_token.at[:, source], a2a_s.at[t], a2a_r.at[t], partner).wait_recv()
    for order in range(2):
        for hf in range(2):
            wpair_wait(order, 0, 0, hf, (order, hf, 0))
    for d, dr, hf in plane_steps(0, True):
        for order in range(2):
            wpair_wait(order, d, dr, hf, (order, hf, 1 + (d - 1) * 2 + dr))

    zrow_all(1 - c).wait_recv()
    w_tiles = width // tile

    def project(i, carry):
        block = w_proj[lax.div(i, w_tiles // n_y), lax.rem(i, w_tiles // n_y)].reshape(n_tp * HEAD_DIM, tile)
        columns = pl.ds(pl.multiple_of(i * tile, tile), tile)
        proj[:, columns] = jnp.dot(by_token[...], block, preferred_element_type=F32)
        return carry

    lax.fori_loop(0, w_tiles, project, 0, unroll=4)

    def norms(i, carry):
        at_rows = pl.ds(pl.multiple_of(i * 16, 16), 16)
        value = proj[at_rows, :]
        scale = lax.rsqrt(jnp.mean(value * value, axis=1, keepdims=True) + EPS)
        mixed_bf = (residual[at_rows, :].astype(F32) + mixer_gain[...] * (value * scale)).astype(BF)
        mixed[at_rows, :] = mixed_bf
        mixed_f = mixed_bf.astype(F32)
        scale = lax.rsqrt(jnp.mean(mixed_f * mixed_f, axis=1, keepdims=True) + EPS)
        normed[at_rows, :] = (mixed_f * scale * expert_gain[...]).astype(BF)
        return carry

    lax.fori_loop(0, tok // 16, norms, 0, unroll=4)

    head = jnp.dot(placing[...], normed[:, 0:128], preferred_element_type=F32)
    send[:, 0:128] = (head + gate_rows[...]).astype(BF)
    send[:, 128:] = jnp.dot(placing[...], normed[:, 128:], preferred_element_type=F32).astype(BF)
    def cut(ch):
        return pl.ds(ch * span, span)

    disp = {}
    for hf in range(2):
        for ch in range(CHUNKS):
            for j in range(hf * half, (hf + 1) * half):
                at_slot = (pl.ds(j * SLOT, SLOT), cut(ch))
                if j > 0:
                    disp[(ch, j)] = push(
                        send.at[at_slot],
                        arr.at[at_slot],
                        disp_s.at[ch, j],
                        disp_r.at[ch, j],
                        (lax.rem(sp + j, n_sp), z, c),
                    )
    arr[0:SLOT] = send[0:SLOT]

    def reach(dr, hf):
        return far if dr == hf else far - 1

    def at(dr, d):
        return (n_z - d) % n_z if dr == 0 else d

    arrivals = [(1, 0), (1, 1)] + [(d, 0) for d in range(2, far + 1)] + [(d, 1) for d in range(2, far)]
    together = [[(0, 0), (0, 1)]]
    for d, kind in arrivals:
        together.append([(at(dr, d), kind if d == 1 or dr == 0 else 1 - kind) for dr in range(2)])
    place_at = {unit: (i, sub) for i, units in enumerate(together) for sub, unit in enumerate(units)}

    def spot(o, rc, hf):
        i, sub = place_at[(o, hf)]
        return i, pl.ds((sub * 2 + rc) * hr, hr)

    def sum_spot(o, hf):
        i, sub = place_at[(o, hf)]
        return i, pl.ds(sub * hr, hr)

    ring = {}
    ring_g = {}
    pair = {}

    def ring_send(dr, d, hf, ch):
        src, dst = at(dr, d), at(dr, d + 1)
        sem = (dr, d, hf, ch)
        ring[sem] = push(
            rows.at[(*spot(src, 0, hf), cut(ch))],
            rows.at[(*spot(dst, 0, hf), cut(ch))],
            ring_s.at[sem],
            ring_r.at[sem],
            ring_dev[dr],
        )
        if ch == 0:
            sem = (dr, d, hf)
            ring_g[sem] = push(
                gates.at[src, 0, hf], gates.at[dst, 0, hf], rgate_s.at[sem], rgate_r.at[sem], ring_dev[dr]
            )

    def ring_wait(dr, d, hf, ch):
        ring[(dr, d - 1, hf, ch)].wait_recv()
        if ch == 0:
            ring_g[(dr, d - 1, hf)].wait_recv()

    def pair_send(o, hf):
        pair[(o, hf)] = (
            push(rows.at[spot(o, 0, hf)], rows.at[spot(o, 1, hf)], pair_s.at[o, hf], pair_r.at[o, hf], partner),
            push(gates.at[o, 0, hf], gates.at[o, 1, hf], pgate_s.at[o, hf], pgate_r.at[o, hf], partner),
        )

    for hf in range(2):
        block = pl.ds(hf * half * SLOT, half * SLOT)
        for ch in range(CHUNKS):
            for j in range(hf * half, (hf + 1) * half):
                if j > 0:
                    disp[(ch, j)].wait_recv()
            if ch == 0:
                gates[0, 0, hf] = jnp.dot(
                    gate_pick[...], arr[block, 0:128], preferred_element_type=F32
                ).astype(BF)
            rows[(*spot(0, 0, hf), cut(ch))] = jnp.dot(
                pick[...], arr[block, cut(ch)], preferred_element_type=F32
            ).astype(BF)
            ring_send(0, 0, hf, ch)
            ring_send(1, 0, hf, ch)
        pair_send(0, hf)

    for load in loads:
        load.wait()

    eye = one_hot(iota((hr, 128), 0) == iota((hr, 128), 1))
    summed = {}

    def compute(step):
        for sub, (o, hf) in enumerate(together[step]):
            for copy in pair[(o, hf)]:
                copy.wait_recv()
            for rc in range(2):
                gcol[pl.ds((sub * 2 + rc) * hr, hr)] = lax.dot_general(
                    eye, gates[o, rc, hf], (((1,), (1,)), ((), ())), preferred_element_type=F32
                )
        for e in range(experts):
            pre = jnp.dot(rows[step], w_in[e], preferred_element_type=F32)
            gate_pre, up_pre = pre[:, :hid], pre[:, hid:]
            scaled = gate_pre / (1.0 + jnp.exp(-gate_pre)) * up_pre * gcol[:, e : e + 1]
            hidden[:, e * hid : (e + 1) * hid] = scaled.astype(BF)

        def down(i, carry):
            columns = pl.ds(pl.multiple_of(i * tile, tile), tile)
            piece = jnp.dot(hidden[...], w_out[:, columns], preferred_element_type=F32).astype(BF)
            for sub in range(2):
                own[step, pl.ds(sub * hr, hr), columns] = piece[sub * 2 * hr : (sub * 2 + 1) * hr]
                oth[step, pl.ds(sub * hr, hr), columns] = piece[(sub * 2 + 1) * hr : (sub * 2 + 2) * hr]
            return carry

        lax.fori_loop(0, width // tile, down, 0, unroll=2)
        summed[step] = push(oth.at[step], got.at[step], sum_s.at[step], sum_r.at[step], partner)

    hops = {}
    settled = set()

    def settle(o, hf):
        step = place_at[(o, hf)][0]
        if step not in settled:
            summed[step].wait_recv()
            settled.add(step)

    def own_rows(o, hf, i):
        step, sub = place_at[(o, hf)]
        return step, pl.ds(pl.multiple_of(sub * hr + i * 16, 16), 16)

    def hop_send(dr, d, hf, ch):
        o = (n_z - d) % n_z if dr == 1 else d
        settle(o, hf)
        start = d == reach(1 - dr, hf)
        if start:
            src = own.at[(*sum_spot(o, hf), cut(ch))]
        else:
            hops[(dr, d + 1, hf, ch)].wait_recv()
            src = hop.at[dr, d, hf, :, cut(ch)]

        def add(i, carry):
            local = pl.ds(pl.multiple_of(i * 16, 16), 16)
            at_rows = (*own_rows(o, hf, i), cut(ch))
            total = own[at_rows].astype(F32) + got[at_rows].astype(F32)
            if not start:
                total = total + hop[dr, d, hf, local, cut(ch)].astype(F32)
            src[local] = total.astype(BF)
            return carry

        lax.fori_loop(0, hr // 16, add, 0)
        sem = (dr, d, hf, ch)
        hops[sem] = push(src, hop.at[dr, d - 1, hf, :, cut(ch)], hop_s.at[sem], hop_r.at[sem], ring_dev[dr])

    returned = {}

    def finish(ch):
        for hf in range(2):
            settle(0, hf)
            for dr in range(2):
                hops[(dr, 1, hf, ch)].wait_recv()

            def last_add(i, carry):
                local = pl.ds(pl.multiple_of(i * 16, 16), 16)
                at_rows = (*own_rows(0, hf, i), cut(ch))
                total = own[at_rows].astype(F32) + got[at_rows].astype(F32)
                total = total + (
                    hop[0, 0, hf, local, cut(ch)].astype(F32) + hop[1, 0, hf, local, cut(ch)].astype(F32)
                )
                own[at_rows] = total.astype(BF)
                return carry

            lax.fori_loop(0, hr // 16, last_add, 0)
            ret[pl.ds(hf * half * SLOT, half * SLOT), cut(ch)] = jnp.dot(
                pick_t[...], own[(*sum_spot(0, hf), cut(ch))], preferred_element_type=F32
            ).astype(BF)
            for j in range(hf * half, (hf + 1) * half):
                at_slot = (pl.ds(j * SLOT, SLOT), cut(ch))
                if j == 0:
                    back[0:SLOT, cut(ch)] = ret[0:SLOT, cut(ch)]
                else:
                    returned[(ch, j)] = push(
                        ret.at[at_slot],
                        back.at[at_slot],
                        ret_s.at[ch, j],
                        ret_r.at[ch, j],
                        (lax.rem(sp + n_sp - j, n_sp), z, c),
                    )

    compute(0)

    def long_hop(d, ch):
        for dr in range(2):
            hop_send(dr, d, 1 - dr, ch)

    done = {0}

    def need(step):
        if step not in done:
            compute(step)
            done.add(step)

    far_step = place_at[(far, 0)][0]
    for k, (d, kind) in enumerate(arrivals):
        step = k + 1
        for ch in range(CHUNKS):
            if step == far_step + 1 and ch == CHUNKS // 2:
                need(far_step)
            for dr in range(2):
                hf = together[step][dr][1]
                ring_wait(dr, d, hf, ch)
                if d < reach(dr, hf) and not (d == 1 and dr != hf):
                    ring_send(dr, d, hf, ch)
        if (d, kind) == (far - 1, 0):
            for ch in range(CHUNKS):
                for dr in range(2):
                    if 1 < reach(dr, 1 - dr):
                        ring_send(dr, 1, 1 - dr, ch)
        for o, hf in together[step]:
            pair_send(o, hf)
        if k > 0 and step != far_step + 1 and step != len(arrivals):
            need(step - 1)
        if step == len(arrivals) - 1 and far > 2:
            for ch in range(CHUNKS):
                long_hop(far, ch)
            need(step)
    if far == 2:
        need(1)
        need(2)
        need(3)
        for ch in range(CHUNKS):
            long_hop(far, ch)
    for ch in range(CHUNKS // 2):
        long_hop(far - 1, ch)
    need(len(arrivals))
    for ch in range(CHUNKS // 2, CHUNKS):
        long_hop(far - 1, ch)
    events = []
    for ch in range(CHUNKS):
        at_key = 1.2 * ch
        for d in range(far - 1, 0, -1):
            events.append((at_key, ch, d, 1))
            at_key += 1
            if d > 1:
                events.append((at_key, ch, d - 1, 0))
                at_key += 1
        events.append((at_key + 0.3, ch, 0, 0))
    for _, ch, d, kind in sorted(events):
        if d == 0:
            finish(ch)
        else:
            for dr in range(2):
                hop_send(dr, d, 1 - dr if kind == 0 else dr, ch)
    eye_tok = one_hot(iota((tok, tok), 0) == iota((tok, tok), 1))
    placing_t = lax.dot_general(
        eye_tok, placing[...], (((1,), (1,)), ((), ())), preferred_element_type=F32
    ).astype(BF)
    for ch in range(CHUNKS):
        for j in range(1, n_sp):
            returned[(ch, j)].wait_recv()
        expert_out = jnp.dot(placing_t, back[:, cut(ch)], preferred_element_type=F32)
        out[:, cut(ch)] = (mixed[:, cut(ch)].astype(F32) + expert_out).astype(BF)
    for t in range(1, n_tp):
        a2a_copy(t, lax.rem(me + t, n_tp)).wait_send()
    zrow_all(c).wait_send()
    for copy in sends:
        copy.wait_send()


def per_device(
    queries,
    key_heads,
    value_heads,
    sink_logit,
    out_weight,
    residual,
    mixer_gain,
    expert_gain,
    route_group,
    route_member,
    route_weight,
    gate_weight,
    up_weight,
    down_weight,
    n_x=4,
    cap=GROUP_CAP,
    kv_share=HEADS // KV_HEADS,
):
    n_sp, n_z = lax.axis_size("sp"), lax.axis_size("tp_0")
    n_y = n_sp // n_x
    n_tp = 2 * n_z
    tok, width = residual.shape
    seq = queries.shape[0]
    experts, hid = down_weight.shape[0], down_weight.shape[1]
    half = n_sp // 2
    hr = half * cap
    far = n_z // 2
    r = np.arange(hr)
    padded = r // cap * SLOT + r % cap
    i = np.arange(half * SLOT)
    e = np.arange(16)
    pick = jnp.asarray(i[None, :] == padded[:, None], BF)
    pick_t = jnp.asarray(i[:, None] == padded[None, :], BF)
    gate_pick = jnp.asarray((i[None, :] % SLOT == e[:, None] + cap) & (e[:, None] < experts), BF)
    vmem = pl.BlockSpec(memory_space=pltpu.VMEM)
    anywhere = pl.BlockSpec(memory_space=pl.ANY)
    dma = pltpu.SemaphoreType.DMA
    bf_bufs = [
        (seq, HEAD_DIM),
        (seq + 2 * WINDOW, HEAD_DIM),
        (seq + 2 * WINDOW, HEAD_DIM),
        (n_tp, BLOCK, HEAD_DIM),
        (tok, n_tp * HEAD_DIM),
        (n_y, n_x // 2, n_z, 2, 128, 256),
        None,
        (tok, width),
        (tok, width),
        (n_sp * SLOT, tok),
        None,
        (n_sp * SLOT, width),
        (n_sp * SLOT, width),
        (n_z, 4 * hr, width),
        (n_z, 2, 2, 16, 128),
        None,
        (4 * hr, experts * hid),
        (experts, width, 2 * hid),
        (experts * hid, width),
        (n_z, 2 * hr, width),
        (n_z, 2 * hr, width),
        (n_z, 2 * hr, width),
        (2, far, 2, hr, width),
        (n_sp * SLOT, width),
        (n_sp * SLOT, width),
    ]
    f32_bufs = iter([(tok, width), (n_sp * SLOT, 128), (4 * hr, 16)])
    buffers = [pltpu.VMEM(s, BF) if s is not None else pltpu.VMEM(next(f32_bufs), F32) for s in bf_bufs]
    sems = [(4,)]
    sems += [(2, 2)] * 2 + [(n_tp,)] * 2 + [(n_z,)] * 2 + [(2, 2, 2, 2)] * 4 + [(2, 2, 5)] * 2
    sems += [(2, far, 2)] * 2 + [(1,)] * 2 + [(width // 256,)]
    sems += [(experts, 3)] + [(CHUNKS, n_sp)] * 2 + [(2, far, 2, CHUNKS)] * 2 + [(2, far, 2)] * 2 + [(n_z, 2)] * 4 + [(n_z,)] * 2
    sems += [(2, far + 1, 2, CHUNKS)] * 2 + [(CHUNKS, n_sp)] * 2
    return pl.pallas_call(
        functools.partial(layer_kernel, n_sp, n_x, n_z, kv_share, cap),
        out_shape=jax.ShapeDtypeStruct((tok, width), BF),
        in_specs=[anywhere] * 3 + [vmem, anywhere] + [vmem] * 9 + [anywhere] * 3,
        out_specs=vmem,
        scratch_shapes=buffers + [dma(s) for s in sems],
        compiler_params=pltpu.CompilerParams(
            collective_id=0, has_side_effects=True, vmem_limit_bytes=VMEM_LIMIT
        ),
    )(
        queries,
        key_heads,
        value_heads,
        sink_logit.reshape(1, 1),
        out_weight,
        residual,
        mixer_gain.reshape(1, -1),
        expert_gain.reshape(1, -1),
        route_group.reshape(1, -1),
        route_member.T,
        route_weight.T,
        pick,
        pick_t,
        gate_pick,
        gate_weight,
        up_weight,
        down_weight,
    )


def solution(mesh):
    torus = Mesh(mesh.devices.reshape(mesh.shape["sp"], 8, 2), ("sp", "tp_0", "tp_1"))
    placed = (
        P("sp", TP),
        P("sp", None),
        P("sp", None),
        P(TP),
        P(TP, None),
        P(SP_TP, None),
        P(),
        P(),
        P(SP_TP),
        P(SP_TP, None),
        P(SP_TP, None),
        P("sp", None, TP),
        P("sp", None, TP),
        P("sp", TP, None),
    )
    return jax.shard_map(
        per_device, mesh=torus, in_specs=placed, out_specs=P(SP_TP, None), check_vma=False
    )
```
